128 devices in a mesh: rep: 2 (over x_hi), fs: 16 (over y, x_lo, core), tp: 4 (over z).
Axes of the slice: x: 4 (x_hi: 2, x_lo: 2; x = x_hi * 2 + x_lo), y: 4, z: 4, core: 2. Of those that a mesh axis runs over, the one named last changes fastest.
Arguments:
- acts: bfloat16 [8192, 2048], P(('rep', 'fs'), 'tp'), may hold values from -6 to 6
- cotangent: bfloat16 [8192, 2048], P(('rep', 'fs'), 'tp'), may hold values from -8 to 8
- pre_act: bfloat16 [8192, 4096], P(('rep', 'fs'), 'tp'), may hold values from -6 to 6
- up_store: float32 [2048, 4096], P('fs', 'tp'), may hold values from -0.125 to 0.125
- up_scale: float32 [4096], P('tp'), may hold values from 0.5 to 2
- down_store: float32 [4096, 2048], P('tp', 'fs'), may hold values from -0.09375 to 0.09375
- down_scale: float32 [2048], replicated, may hold values from 0.5 to 2
Outputs:
- grad_input: bfloat16 [8192, 2048], P(('rep', 'fs'), 'tp')
- grad_up: float32 [2048, 4096], P('fs', 'tp')
- grad_down: float32 [4096, 2048], P('tp', 'fs')
The draws below stay inside these ranges and needn't reach their ends.
All inputs are finite; a program needn't handle non-finite values.
Results may differ from the reference program's by a relative error of at most 0.007.
Values may be sent and summed in bfloat16 or wider, within the bound.
A program may use at most 128 MiB of HBM per device.

```python
import math
import jax
import jax.numpy as jnp

D = 2048
FF = 4096
TOKENS = 8192


def with_spikes(entries, rng, source, target, blocks, factor):
    owner, partner = [(jnp.arange(entries.shape[dim]) // (entries.shape[dim] // blocks)).reshape([-1 if axis == dim else 1 for axis in range(entries.ndim)]) for dim in (source, target)]
    chosen = jax.random.permutation(rng, blocks)[partner]
    strong = (owner == chosen) | (owner == (partner + blocks // 2) % blocks)
    return jnp.where(strong, factor * entries, entries)


def block_scale(own_key, shape, split, smallest, high):
    gain, own = 1.0, jax.random.fold_in(own_key, 6)
    for axis_at, parts in split:
        draws = jnp.exp(jax.random.uniform(jax.random.fold_in(own, axis_at), (parts,), jnp.float32, smallest / len(split), high / len(split)))
        gain = gain * jnp.repeat(draws, shape[axis_at] // parts).reshape([-1 if axis == axis_at else 1 for axis in range(len(shape))])
    return gain


def noise(stream_key, shape, scale, limit, pieces=(), kind=jnp.bfloat16):
    result = jax.random.normal(stream_key, shape, jnp.float32) * scale
    if len(pieces) > 0:
        result = block_scale(stream_key, shape, pieces, -0.22, 0.18) * result
    return jnp.clip(result, min=-limit, max=limit).astype(kind)


def gaussian_with(key, dims, spread, bound, cuts, heavy, dtype=jnp.bfloat16):
    array = spread * jax.random.normal(key, dims, jnp.float32)
    if cuts:
        array = array * block_scale(key, dims, cuts, -0.22, 0.18)
    return jnp.clip(with_spikes(array, jax.random.fold_in(key, 3), *heavy), -bound, bound).astype(dtype)


def setup_inputs(seed: int = 0) -> dict:
    arg_keys = jax.random.split(jax.random.key(seed), 8)
    return {
        "acts": noise(arg_keys[0], (TOKENS, D), 1.0, 6.0, ((0, 32), (1, 4))),
        "cotangent": gaussian_with(arg_keys[1], (TOKENS, D), 1.0, 8.0, ((0, 32), (1, 4)), (0, 1, 32, 2.75)),
        "pre_act": noise(arg_keys[2], (TOKENS, FF), 1.0, 6.0, ((0, 32), (1, 4))),
        "up_store": noise(arg_keys[3], (D, FF), D ** -0.5, 0.125, ((0, 16), (1, 4)), jnp.float32),
        "up_scale": jnp.clip(jnp.exp(math.log(2.0) - 1.3862944 * jax.random.uniform(arg_keys[4], (FF,), jnp.float32) ** block_scale(arg_keys[4], (FF,), ((0, 4),), -0.2, 0.2)), 0.5, 2.0),
        "down_store": noise(arg_keys[5], (FF, D), FF ** -0.5, 0.09375, ((0, 4), (1, 16)), jnp.float32),
        "down_scale": jnp.clip(jnp.exp(jax.random.uniform(arg_keys[6], (D,), jnp.float32, math.log(0.5), math.log(2.0))), 0.5, 2.0),
    }


def reference(acts, cotangent, pre_act, up_store, up_scale, down_store, down_scale):
    norm_factor = 1.0 / math.sqrt(TOKENS)
    scaled = (cotangent.astype(jnp.float32) * down_scale[None, :]).astype(jnp.bfloat16)
    d_act = jnp.dot(scaled, down_store.astype(jnp.bfloat16).T, preferred_element_type=jnp.float32)
    positive = jnp.maximum(pre_act.astype(jnp.float32), 0.0)
    act = (positive * positive).astype(jnp.bfloat16)
    d_pre = (2.0 * positive * d_act * up_scale[None, :]).astype(jnp.bfloat16)
    grad_down = jnp.dot(act.T, scaled, preferred_element_type=jnp.float32) * norm_factor
    grad_up = jnp.dot(acts.T, d_pre, preferred_element_type=jnp.float32) * norm_factor
    grad_input = jnp.dot(d_pre, up_store.astype(jnp.bfloat16).T, preferred_element_type=jnp.float32).astype(jnp.bfloat16)
    return (grad_input, grad_up, grad_down)
```

```python
import math

import jax
import jax.numpy as jnp
from jax import lax
from jax.experimental import pallas as pl
from jax.experimental.pallas import tpu as pltpu
from jax.sharding import PartitionSpec as P

BF = jnp.bfloat16
F32 = jnp.float32
MESH = pl.DeviceIdType.MESH
COPIES = 96


def nt(a, b):
    return lax.dot_general(a, b, (((1,), (1,)), ((), ())), preferred_element_type=F32)


def nn(a, b):
    return lax.dot_general(a, b, (((1,), (0,)), ((), ())), preferred_element_type=F32)


def kernel(
    norm, cot, acts, pre, up, ups, down, dsc,
    gi_out, gu_out, gd_out,
    loc_s, loc_a, xs, xa, pre_r, act_t, wd, wu, da, dr, dpre,
    pd, rxd, sd, y2pd, y2md, ypd, ymd, fd, rrd,
    pu, rxu, su, y2pu, y2mu, ypu, ymu, fu, rru,
    gi, z2p, z2m, zp, zm, fz, rd,
    ssem, rsem,
):
    r, f, z = (lax.axis_index(n) for n in ("rep", "fs", "tp"))
    y = lax.div(f, 4)
    xl = lax.rem(lax.div(f, 2), 2)
    c = lax.rem(f, 2)
    x = r * 2 + xl
    oc, ox = 1 - c, 1 - xl

    def dev(dx=0, dy=0, dz=0, core=None):
        nx, ny, nz = (lax.rem(a + d + 4, 4) for a, d in ((x, dx), (y, dy), (z, dz)))
        core = c if core is None else core
        return {
            "rep": lax.div(nx, 2),
            "fs": ny * 4 + lax.rem(nx, 2) * 2 + core,
            "tp": nz,
        }

    def at(a, d):
        return lax.rem(a + d + 4, 4)

    barrier = pltpu.get_barrier_semaphore()
    peers = [dev(dz=d, core=k) for d in (1, -1) for k in (c, oc)]
    peers += [dev(dy=1), dev(dy=-1), dev(dx=1), dev(dx=-1), dev(dx=2), dev(core=oc)]
    for p in peers:
        pl.semaphore_signal(barrier, inc=1, device_id=p, device_id_type=MESH)

    started = []

    def send(src, dst, to):
        k = len(started)
        copy = pltpu.make_async_remote_copy(
            src_ref=src, dst_ref=dst, send_sem=ssem.at[k], recv_sem=rsem.at[k],
            device_id=to, device_id_type=MESH,
        )
        copy.start()
        started.append(copy)
        return copy

    scale = dsc[:, pl.ds(pl.multiple_of(z * 512, 512), 512)]
    scaled = (cot[...].astype(F32) * scale).astype(BF)
    for k in range(2):
        for j in range(2):
            lanes = slice(j * 256 + k * 128, j * 256 + k * 128 + 128)
            loc_s[k, :, j * 128:(j + 1) * 128] = scaled[:, lanes]
            loc_a[k, :, j * 128:(j + 1) * 128] = acts[:, lanes]
    wd[y, xl] = down[...].astype(BF)
    wu[y, xl] = up[...].astype(BF)
    xs[z, 0:256, :] = loc_s[c]
    xa[z, 0:256, :] = loc_a[c]
    pl.semaphore_wait(barrier, len(peers))

    own, other = pl.ds(0, 256), pl.ds(256, 256)

    def z_send(loc, full):
        out = []
        for d in (1, -1):
            out.append(send(loc.at[c], full.at[z, own, :], dev(dz=d)))
            out.append(send(loc.at[oc], full.at[z, other, :], dev(dz=d, core=oc)))
        out.append(send(loc.at[oc], full.at[z, other, :], dev(core=oc)))
        return out

    def z_forward(full, first):
        first[0].wait_recv()
        a = send(full.at[at(z, -1), own, :], full.at[at(z, -1), own, :], dev(dz=1))
        first[3].wait_recv()
        b = send(full.at[at(z, 1), other, :], full.at[at(z, 1), other, :], dev(dz=-1))
        return [first[1], first[2], first[4], a, b]

    def half(ref, k, xx, h):
        rows = ref.shape[2] // 2
        return ref.at[k, xx, pl.ds(h * rows, rows), :]

    def x_send(w, k, h):
        return send(half(w, k, xl, h), half(w, k, xl, h), dev(dx=1 - 2 * h))

    def w_first(w):
        return [send(w.at[y, xl], w.at[y, xl], dev(dy=d)) for d in (1, -1)]

    def w_second(w, first):
        fwd = []
        xsend = []
        for h, d in ((0, 1), (1, -1)):
            first[h].wait_recv()
            k = at(y, -d)
            fwd.append(send(half(w, k, xl, h), half(w, k, xl, h), dev(dy=d)))
            xsend += [x_send(w, k, 0), x_send(w, k, 1)]
        return fwd, xsend

    def w_third(w, fwd):
        xsend = []
        for h in range(2):
            fwd[h].wait_recv()
            xsend.append(x_send(w, at(y, 2), h))
        return xsend

    def wait_recv(copies):
        for k in copies:
            k.wait_recv()

    s1 = z_send(loc_s, xs)
    wd1 = w_first(wd)
    wdx = [x_send(wd, y, 0), x_send(wd, y, 1)]
    pre1 = send(pre, pre_r, dev(core=oc))
    s2 = z_forward(xs, s1)
    a1 = z_send(loc_a, xa)
    wd2, more = w_second(wd, wd1)
    wdx += more
    wu1 = w_first(wu)
    wux = [x_send(wu, y, 0), x_send(wu, y, 1)]

    def relu_sq(v):
        p = jnp.maximum(v.astype(F32), 0.0)
        return (p * p).astype(BF)

    act_t[:, 0:256] = relu_sq(pre[...]).T
    pre1.wait_recv()
    act_t[:, 256:512] = relu_sq(pre_r[...]).T
    wait_recv(s2)
    wdx += w_third(wd, wd2)

    for k in range(4):
        part = nn(act_t[...], xs[k])
        for j in range(2):
            pd[k, j] = part[:, j * 128:(j + 1) * 128].astype(BF)
    order = (2, 1, -1, 0)

    def scatter_x(part, rx):
        out = {}
        for d in order:
            k = at(y, d)
            out[d] = []
            for h in range(2):
                rows = part.shape[2] // 2
                out[d].append(
                    send(half(part, k, ox, h), rx.at[k, pl.ds(h * rows, rows), :], dev(dx=1 - 2 * h))
                )
        return out

    dx = scatter_x(pd, rxd)
    a2 = z_forward(xa, a1)
    wu2, more = w_second(wu, wu1)
    wux += more

    wait_recv(wdx)
    dax = []
    for h in range(2):
        total = None
        for k in range(4):
            w = jnp.concatenate([wd[k, 0], wd[k, 1]], axis=1)
            term = nt(xs[k, h * 256:(h + 1) * 256, :], w)
            total = term if total is None else total + term
        da[h] = total
        dax.append(send(da.at[h], dr.at[1 - h], dev(core=oc)))
    wux += w_third(wu, wu2)
    wait_recv(a2)
    for h in (1, 0):
        dax[1 - h].wait_recv()
        src = pre if h == 0 else pre_r
        pos = jnp.maximum(src[...].astype(F32), 0.0)
        dpre[h * 256:(h + 1) * 256, :] = (2.0 * pos * (da[h] + dr[h]) * ups[...]).astype(BF)

    for k in range(4):
        part = nn(xa[k].T, dpre[...])
        for j in range(2):
            pu[k, j] = part[j * 128:(j + 1) * 128, :].astype(BF)
    ux = scatter_x(pu, rxu)

    def add(a, b):
        return a.astype(F32) + b.astype(F32)

    def sum_x(part, rx, s, xcopies, d):
        wait_recv(xcopies[d])
        k = at(y, d)
        s[k] = add(part[k, xl], rx[k]).astype(BF)

    def ring_far(s, me, r2p, r2m, nxt, prv):
        n = s.shape[1] // 2
        k = at(me, 2)
        return [
            send(s.at[k, pl.ds(0, n), :], r2p, nxt),
            send(s.at[k, pl.ds(n, n), :], r2m, prv),
        ]

    def ring_near(s, me, far, r2p, r2m, rp, rm, nxt, prv):
        n = s.shape[1] // 2
        out = []
        kp, km = at(me, 1), at(me, -1)
        out.append(send(s.at[kp, pl.ds(n, n), :], rp.at[pl.ds(n, n), :], nxt))
        out.append(send(s.at[km, pl.ds(0, n), :], rm.at[pl.ds(0, n), :], prv))
        far[0].wait_recv()
        s[kp, 0:n, :] = add(s[kp, 0:n, :], r2p[...]).astype(BF)
        out.append(send(s.at[kp, pl.ds(0, n), :], rp.at[pl.ds(0, n), :], nxt))
        far[1].wait_recv()
        s[km, n:, :] = add(s[km, n:, :], r2m[...]).astype(BF)
        out.append(send(s.at[km, pl.ds(n, n), :], rm.at[pl.ds(n, n), :], prv))
        return out

    ypn, ymn, zpn, zmn = dev(dy=1), dev(dy=-1), dev(dz=1), dev(dz=-1)
    sum_x(pd, rxd, sd, dx, 2)
    dfar = ring_far(sd, y, y2pd, y2md, ypn, ymn)
    sum_x(pd, rxd, sd, dx, 1)
    sum_x(pd, rxd, sd, dx, -1)

    wait_recv(wux)
    for k in range(4):
        w = wu[k].reshape(256, 1024)
        gi[k] = nt(dpre[...], w).astype(BF)
    zfar = ring_far(gi, z, z2p, z2m, zpn, zmn)
    dnear = ring_near(sd, y, dfar, y2pd, y2md, ypd, ymd, ypn, ymn)
    sum_x(pd, rxd, sd, dx, 0)
    znear = ring_near(gi, z, zfar, z2p, z2m, zp, zm, zpn, zmn)

    sum_x(pu, rxu, su, ux, 2)
    ufar = ring_far(su, y, y2pu, y2mu, ypn, ymn)
    sum_x(pu, rxu, su, ux, 1)
    sum_x(pu, rxu, su, ux, -1)

    wait_recv(dnear)
    fd[...] = (add(sd[y], ypd[...]) + ymd[...].astype(F32)).astype(BF)
    drep = send(fd, rrd, dev(dx=2))

    unear = ring_near(su, y, ufar, y2pu, y2mu, ypu, ymu, ypn, ymn)
    sum_x(pu, rxu, su, ux, 0)

    wait_recv(znear)
    fz[...] = (add(gi[z], zp[...]) + zm[...].astype(F32)).astype(BF)
    dz = send(fz.at[other, :], rd, dev(core=oc))

    wait_recv(unear)
    fu[...] = (add(su[y], ypu[...]) + ymu[...].astype(F32)).astype(BF)
    urep = send(fu, rru, dev(dx=2))

    dz.wait_recv()
    for j in range(2):
        lanes = pl.ds(pl.multiple_of(j * 256 + c * 128, 128), 128)
        gi_out[:, lanes] = fz[0:256, j * 128:(j + 1) * 128]
        lanes = pl.ds(pl.multiple_of(j * 256 + oc * 128, 128), 128)
        gi_out[:, lanes] = rd[:, j * 128:(j + 1) * 128]
    drep.wait_recv()
    gd_out[...] = add(fd[...], rrd[...]) * norm
    urep.wait_recv()
    gu_out[...] = add(fu[...], rru[...]) * norm
    for copy in started:
        copy.wait_send()


def body(acts, cotangent, pre_act, up_store, up_scale, down_store, down_scale):
    tokens = acts.shape[0] * lax.axis_size("fs") * lax.axis_size("rep")
    norm = 1.0 / math.sqrt(tokens)

    def vm(*shape, dtype=BF):
        return pltpu.VMEM(shape, dtype)

    def grad_bufs(a, b):
        h = a // 2
        return [
            vm(4, 2, a, b), vm(4, a, b), vm(4, a, b), vm(h, b), vm(h, b),
            vm(a, b), vm(a, b), vm(a, b), vm(a, b),
        ]

    spec = pl.BlockSpec(memory_space=pltpu.VMEM)

    def call(*args):
        return kernel(norm, *args)

    return pl.pallas_call(
        call,
        name="ffn_backward",
        out_shape=(
            jax.ShapeDtypeStruct((256, 512), BF),
            jax.ShapeDtypeStruct((128, 1024), F32),
            jax.ShapeDtypeStruct((1024, 128), F32),
        ),
        in_specs=[spec] * 7,
        out_specs=(spec,) * 3,
        scratch_shapes=[
            vm(2, 256, 256), vm(2, 256, 256), vm(4, 512, 256), vm(4, 512, 256),
            vm(256, 1024), vm(1024, 512), vm(4, 2, 1024, 128), vm(4, 2, 128, 1024),
            vm(2, 256, 1024, dtype=F32), vm(2, 256, 1024, dtype=F32), vm(512, 1024),
            *grad_bufs(1024, 128),
            *grad_bufs(128, 1024),
            vm(4, 512, 256), vm(256, 256), vm(256, 256), vm(512, 256), vm(512, 256),
            vm(512, 256), vm(256, 256),
            pltpu.SemaphoreType.DMA((COPIES,)),
            pltpu.SemaphoreType.DMA((COPIES,)),
        ],
        compiler_params=pltpu.CompilerParams(
            collective_id=0, has_side_effects=True, vmem_limit_bytes=56 * 1024 * 1024
        ),
    )(
        cotangent, acts, pre_act, up_store, up_scale.reshape(1, -1),
        down_store, down_scale.reshape(1, -1),
    )


def solution(mesh):
    return jax.shard_map(
        body,
        mesh=mesh,
        in_specs=(
            P(("rep", "fs"), "tp"),
            P(("rep", "fs"), "tp"),
            P(("rep", "fs"), "tp"),
            P("fs", "tp"),
            P("tp"),
            P("tp", "fs"),
            P(),
        ),
        out_specs=(P(("rep", "fs"), "tp"), P("fs", "tp"), P("tp", "fs")),
        check_vma=False,
    )
```

```python
import math

import jax
import jax.numpy as jnp
from jax import lax
from jax.experimental import pallas as pl
from jax.experimental.pallas import tpu as pltpu
from jax.sharding import PartitionSpec as P

BF = jnp.bfloat16
F32 = jnp.float32
MESH = pl.DeviceIdType.MESH
COPIES = 128


def nt(a, b):
    return lax.dot_general(a, b, (((1,), (1,)), ((), ())), preferred_element_type=F32)


def nn(a, b):
    return lax.dot_general(a, b, (((1,), (0,)), ((), ())), preferred_element_type=F32)


def kernel(
    norm, cot, acts, pre, up, ups, down, dsc,
    gi_out, gu_out, gd_out,
    loc_s, loc_a, xs, xa, pre_r, act_t, wd, wu, da, dr, dpre,
    pd, td1, td2, fd, rd, farxd, nearxd, farxd2, nearxd2, faryd, nearyd, faryd2, nearyd2,
    pu, tu1, tu2, fu, ru, farxu, nearxu, farxu2, nearxu2, faryu, nearyu, faryu2, nearyu2,
    gi, farz, nearz, fz, rz,
    ssem, rsem,
):
    r, f, z = (lax.axis_index(n) for n in ("rep", "fs", "tp"))
    y = lax.div(f, 4)
    xl = lax.rem(lax.div(f, 2), 2)
    c = lax.rem(f, 2)
    x = r * 2 + xl
    oc, ox = 1 - c, 1 - xl

    def dev(dx=0, dy=0, dz=0, core=None):
        nx, ny, nz = (lax.rem(a + d + 4, 4) for a, d in ((x, dx), (y, dy), (z, dz)))
        core = c if core is None else core
        return {
            "rep": lax.div(nx, 2),
            "fs": ny * 4 + lax.rem(nx, 2) * 2 + core,
            "tp": nz,
        }

    def at(a, d):
        return lax.rem(a + d + 4, 4)

    barrier = pltpu.get_barrier_semaphore()
    peers = [dev(dz=d, core=k) for d in (1, -1) for k in (c, oc)]
    peers += [dev(dy=1), dev(dy=-1), dev(dx=1), dev(dx=-1), dev(dx=2), dev(core=oc)]
    for p in peers:
        pl.semaphore_signal(barrier, inc=1, device_id=p, device_id_type=MESH)

    started = []

    def send(src, dst, to):
        k = len(started)
        copy = pltpu.make_async_remote_copy(
            src_ref=src, dst_ref=dst, send_sem=ssem.at[k], recv_sem=rsem.at[k],
            device_id=to, device_id_type=MESH,
        )
        copy.start()
        started.append(copy)
        return copy

    scale = dsc[:, pl.ds(pl.multiple_of(z * 512, 512), 512)]
    scaled = (cot[...].astype(F32) * scale).astype(BF)
    for k in range(2):
        for j in range(2):
            lanes = slice(j * 256 + k * 128, j * 256 + k * 128 + 128)
            loc_s[k, :, j * 128:(j + 1) * 128] = scaled[:, lanes]
            loc_a[k, :, j * 128:(j + 1) * 128] = acts[:, lanes]
    wd[y, xl] = down[...].astype(BF)
    wu[y, xl] = up[...].astype(BF)
    xs[z, 0:256, :] = loc_s[c]
    xa[z, 0:256, :] = loc_a[c]
    pl.semaphore_wait(barrier, len(peers))

    own, other = pl.ds(0, 256), pl.ds(256, 256)

    def z_send(loc, full):
        out = []
        for d in (1, -1):
            out.append(send(loc.at[c], full.at[z, own, :], dev(dz=d)))
            out.append(send(loc.at[oc], full.at[z, other, :], dev(dz=d, core=oc)))
        out.append(send(loc.at[oc], full.at[z, other, :], dev(core=oc)))
        return out

    def z_forward(full, first):
        first[0].wait_recv()
        a = send(full.at[at(z, -1), own, :], full.at[at(z, -1), own, :], dev(dz=1))
        first[3].wait_recv()
        b = send(full.at[at(z, 1), other, :], full.at[at(z, 1), other, :], dev(dz=-1))
        return [first[1], first[2], first[4], a, b]

    def wait_recv(copies):
        for k in copies:
            k.wait_recv()

    def add(a, b):
        return a.astype(F32) + b.astype(F32)

    def relu_sq(v):
        p = jnp.maximum(v.astype(F32), 0.0)
        return (p * p).astype(BF)

    def rows_of(ref, k, xx, lo, n):
        return ref.at[k, xx, pl.ds(lo, n), :]

    def same(ref, to):
        return send(ref, ref, to)

    yn, yp, xn, xp, zn, zp = dev(dy=1), dev(dy=-1), dev(dx=1), dev(dx=-1), dev(dz=1), dev(dz=-1)

    def x_send(w, lo, n, k, h):
        return same(rows_of(w, k, xl, lo + h * n, n), xp if h else xn)

    class Ring:
        def __init__(self, view, me, far, near, nxt, prv):
            self.view, self.me, self.far, self.near = view, me, far, near
            self.nxt, self.prv = nxt, prv

        def start_far(self):
            k = at(self.me, 2)
            self.f = [
                send(self.view(k, 0), self.far.at[0], self.nxt),
                send(self.view(k, 1), self.far.at[1], self.prv),
            ]

        def start_near(self):
            self.n = [
                send(self.view(at(self.me, 1), 1), self.near.at[0, 1], self.nxt),
                send(self.view(at(self.me, -1), 0), self.near.at[1, 0], self.prv),
            ]

        def mid(self):
            for h, d, to in ((0, 1, self.nxt), (1, -1, self.prv)):
                self.f[h].wait_recv()
                v = self.view(at(self.me, d), h)
                v[...] = add(v[...], self.far[h]).astype(BF)
                self.n.append(send(v, self.near.at[h, h], to))

        def result(self):
            wait_recv(self.n)
            for h in range(2):
                v = self.view(self.me, h)
                yield h, add(v[...], self.near[0, h]) + self.near[1, h].astype(F32)

    class Grad:
        def __init__(self, p, t1, t2, fin, rr, farx, nearx, farx2, nearx2, fary, neary, fary2, neary2):
            n = fin.shape[1] // 2
            self.p, self.t1, self.t2, self.fin, self.rr = p, t1, t2, fin, rr
            self.x1 = Ring(
                lambda k, h: p.at[pl.ds(2 * h, 2), lax.rem(k, 2), 0, lax.div(k, 2)],
                x, farx, nearx, xn, xp,
            )
            self.y1 = Ring(lambda k, h: p.at[k, h, 1], y, fary, neary, yn, yp)
            self.y2 = Ring(
                lambda k, h: t1.at[k, pl.ds(h * n, n), :], y, fary2, neary2, yn, yp
            )
            self.x2 = Ring(
                lambda k, h: t2.at[lax.rem(k, 2), lax.div(k, 2), pl.ds(h * n, n), :],
                x, farx2, nearx2, xn, xp,
            )
            self.n = n

        def start(self):
            self.y1.start_far()
            self.x1.start_far()
            self.y1.start_near()
            self.x1.start_near()

        def mid(self):
            self.y1.mid()
            self.x1.mid()

        def second_y(self):
            for h, v in self.x1.result():
                self.t1[2 * h:2 * h + 2] = v.astype(BF)
            self.y2.start_far()
            self.y2.start_near()

        def second_x(self):
            for h, v in self.y1.result():
                self.t2[h] = v.astype(BF)
            self.x2.start_far()
            self.x2.start_near()

        def second_mid(self):
            self.x2.mid()
            self.y2.mid()

        def share(self):
            self.g = []
            for j, ring in ((1, self.x2), (0, self.y2)):
                for h, v in ring.result():
                    self.fin[j, h * self.n:(h + 1) * self.n, :] = v.astype(BF)
                self.g.append(send(self.fin.at[j], self.rr.at[j], dev(dx=2)))

        def store(self, out):
            for j in range(2):
                out[j, r] = self.fin[j].astype(F32) * norm
            wait_recv(self.g)
            for j in range(2):
                out[j, 1 - r] = self.rr[j].astype(F32) * norm

    gd = Grad(pd, td1, td2, fd, rd, farxd, nearxd, farxd2, nearxd2, faryd, nearyd, faryd2, nearyd2)
    gu = Grad(pu, tu1, tu2, fu, ru, farxu, nearxu, farxu2, nearxu2, faryu, nearyu, faryu2, nearyu2)
    scope = jax.named_scope

    with scope("a_first_sends"):
        s1 = z_send(loc_s, xs)
        wd1 = [
            same(rows_of(wd, y, xl, 512 * h, 512), to)
            for h, to in ((0, yn), (1, yp), (1, yn), (0, yp))
        ]
        wdx = {d: [] for d in (0, 1, -1, 2)}
        wdx[0] = [x_send(wd, 0, 512, y, h) for h in range(2)]
        pre1 = send(pre, pre_r, dev(core=oc))
        wu_x = [x_send(wu, 64, 32, y, h) for h in range(2)]
    with scope("b_wd_first"):
        wd1[0].wait_recv()
        wd2 = [same(rows_of(wd, at(y, -1), xl, 0, 512), yn)]
        wdx[-1].append(x_send(wd, 0, 512, at(y, -1), 0))
        wd1[1].wait_recv()
        wd2.append(same(rows_of(wd, at(y, 1), xl, 512, 512), yp))
        wdx[1].append(x_send(wd, 0, 512, at(y, 1), 1))
    with scope("c_z_forward"):
        s2 = z_forward(xs, s1)
        a1 = z_send(loc_a, xa)
    with scope("d_wd_second"):
        wd1[2].wait_recv()
        wdx[-1].append(x_send(wd, 0, 512, at(y, -1), 1))
        wd1[3].wait_recv()
        wdx[1].append(x_send(wd, 0, 512, at(y, 1), 0))
        wuy = [same(rows_of(wu, y, xl, 0, 64), to) for to in (yn, yp)]
        wuo = [same(rows_of(wu, y, xl, 64, 64), to) for to in (yn, yp)]
    with scope("e_act"):
        act_t[:, 0:256] = relu_sq(pre[...]).T
        pre1.wait_recv()
        act_t[:, 256:512] = relu_sq(pre_r[...]).T
    with scope("f_wd_third"):
        for h in range(2):
            wd2[h].wait_recv()
            wdx[2].append(x_send(wd, 0, 512, at(y, 2), h))
    with scope("g_scaled_wait"):
        wait_recv(s2)
    with scope("h_grad_down"):
        for k in range(4):
            part = nn(act_t[...], xs[k])
            for j in range(2):
                pd[k, j] = part[:, j * 128:(j + 1) * 128].astype(BF).reshape(2, 2, 256, 128)
        gd.start()
    with scope("i_wu_second"):
        wux = [x_send(wu, 0, 32, y, h) for h in range(2)]
        wuo2 = []
        for h in range(2):
            wu_x[h].wait_recv()
            piece = rows_of(wu, y, ox, 64 + 32 * h, 32)
            wuo2 += [same(piece, yn), same(piece, yp)]
        wuf = []
        for h, to, d in ((0, yn, -1), (1, yp, 1)):
            wuy[h].wait_recv()
            k = at(y, d)
            wuf.append(same(rows_of(wu, k, xl, 32 * h, 32), to))
            wux += [x_send(wu, 0, 32, k, 0), x_send(wu, 0, 32, k, 1)]
    with scope("j_acts_forward"):
        a2 = z_forward(xa, a1)
    dax = []
    for d in (0, 1, -1, 2):
        with scope("k_wd_wait"):
            wait_recv(wdx[d])
        with scope("l_d_act"):
            k = at(y, d)
            w = jnp.concatenate([wd[k, 0], wd[k, 1]], axis=1)
            for h in (0, 1):
                term = nt(xs[k, h * 256:(h + 1) * 256, :], w)
                da[h] = term if d == 0 else da[h] + term
                if d == 2:
                    dax.append(send(da.at[h], dr.at[1 - h], dev(core=oc)))
    with scope("m_wu_third"):
        wuo[0].wait_recv()
        wug = [same(rows_of(wu, at(y, -1), xl, 64, 64), yn)]
        for h in range(2):
            wuo2[2 * h + 1].wait_recv()
            wug.append(same(rows_of(wu, at(y, 1), ox, 64 + 32 * h, 32), yp))
        for h in range(2):
            wuf[h].wait_recv()
            wux.append(x_send(wu, 0, 32, at(y, 2), h))
    with scope("n_dpre"):
        for h in (1, 0):
            dax[1 - h].wait_recv()
            src = pre if h == 0 else pre_r
            pos = jnp.maximum(src[...].astype(F32), 0.0)
            dpre[h * 256:(h + 1) * 256, :] = (2.0 * pos * (da[h] + dr[h]) * ups[...]).astype(BF)
    with scope("o_acts_wait"):
        wait_recv(a2)
    with scope("p_grad_up"):
        for k in range(4):
            part = nn(xa[k].T, dpre[...])
            for j in range(2):
                pu[k, j] = part[j * 128:(j + 1) * 128, :].astype(BF).reshape(2, 2, 32, 1024)
        gu.start()
    with scope("q_gd_mid"):
        gd.mid()
    with scope("r_wu_wait"):
        wait_recv(wux)
        wait_recv(wuo[1:] + [wuo2[0], wuo2[2]] + wug)
    zr = Ring(lambda k, h: gi.at[k, pl.ds(256 * h, 256), :], z, farz, nearz, zn, zp)
    with scope("s_grad_in"):
        for d in (2, 1, -1, 0):
            k = at(z, d)
            gi[k] = nt(dpre[...], wu[k].reshape(256, 1024)).astype(BF)
            if d == 2:
                zr.start_far()
            if d == -1:
                zr.start_near()
    with scope("t_gd_second"):
        gd.second_x()
        gd.second_y()
    with scope("u_gu_mid"):
        gu.mid()
    with scope("v_z_mid"):
        zr.mid()
    with scope("w_gd_second_mid"):
        gd.second_mid()
    with scope("x_gu_second"):
        gu.second_x()
        gu.second_y()
    with scope("y_gd_share"):
        gd.share()
    with scope("z_gi"):
        for h, v in zr.result():
            fz[h] = v.astype(BF)
        gx = send(fz.at[1], rz, dev(core=oc))
    with scope("za_gu_second_mid"):
        gu.second_mid()
    with scope("zb_gi_out"):
        gx.wait_recv()
        for j in range(2):
            lanes = pl.ds(pl.multiple_of(j * 256 + c * 128, 128), 128)
            gi_out[:, lanes] = fz[0, :, j * 128:(j + 1) * 128]
            lanes = pl.ds(pl.multiple_of(j * 256 + oc * 128, 128), 128)
            gi_out[:, lanes] = rz[:, j * 128:(j + 1) * 128]
    with scope("zc_gd_out"):
        gd.store(gd_out)
    with scope("zd_gu_share"):
        gu.share()
    with scope("ze_gu_out"):
        gu.store(gu_out)
    with scope("zf_drain"):
        for copy in started:
            copy.wait_send()


def body(acts, cotangent, pre_act, up_store, up_scale, down_store, down_scale):
    tokens = acts.shape[0] * lax.axis_size("fs") * lax.axis_size("rep")
    norm = 1.0 / math.sqrt(tokens)

    def vm(*shape, dtype=BF):
        return pltpu.VMEM(shape, dtype)

    def grad_bufs(n, m):
        out = [vm(4, 2, 2, 2, n, m), vm(4, n, m), vm(2, 2, n, m), vm(2, n, m), vm(2, n, m)]
        for lead, rows in (((2,), n), ((), n // 2)) * 2:
            out += [vm(2, *lead, rows, m), vm(2, 2, *lead, rows, m)]
        return out

    spec = pl.BlockSpec(memory_space=pltpu.VMEM)

    def call(*args):
        return kernel(norm, *args)

    gi, gu, gd = pl.pallas_call(
        call,
        name="ffn_backward",
        out_shape=(
            jax.ShapeDtypeStruct((256, 512), BF),
            jax.ShapeDtypeStruct((2, 2, 32, 1024), F32),
            jax.ShapeDtypeStruct((2, 2, 256, 128), F32),
        ),
        in_specs=[spec] * 7,
        out_specs=(spec,) * 3,
        scratch_shapes=[
            vm(2, 256, 256), vm(2, 256, 256), vm(4, 512, 256), vm(4, 512, 256),
            vm(256, 1024), vm(1024, 512), vm(4, 2, 1024, 128), vm(4, 2, 128, 1024),
            vm(2, 256, 1024, dtype=F32), vm(2, 256, 1024, dtype=F32), vm(512, 1024),
            *grad_bufs(256, 128),
            *grad_bufs(32, 1024),
            vm(4, 512, 256), vm(2, 256, 256), vm(2, 2, 256, 256), vm(2, 256, 256), vm(256, 256),
            pltpu.SemaphoreType.DMA((COPIES,)),
            pltpu.SemaphoreType.DMA((COPIES,)),
        ],
        compiler_params=pltpu.CompilerParams(
            collective_id=0, has_side_effects=True, vmem_limit_bytes=56 * 1024 * 1024
        ),
    )(
        cotangent, acts, pre_act, up_store, up_scale.reshape(1, -1),
        down_store, down_scale.reshape(1, -1),
    )
    return gi, gu.reshape(up_store.shape), gd.reshape(down_store.shape)


def solution(mesh):
    return jax.shard_map(
        body,
        mesh=mesh,
        in_specs=(
            P(("rep", "fs"), "tp"),
            P(("rep", "fs"), "tp"),
            P(("rep", "fs"), "tp"),
            P("fs", "tp"),
            P("tp"),
            P("tp", "fs"),
            P(),
        ),
        out_specs=(P(("rep", "fs"), "tp"), P("fs", "tp"), P("tp", "fs")),
        check_vma=False,
    )
```

```python
import math

import jax
import jax.numpy as jnp
from jax import lax
from jax.experimental import pallas as pl
from jax.experimental.pallas import tpu as pltpu
from jax.sharding import PartitionSpec as P

BF = jnp.bfloat16
F32 = jnp.float32
MESH = pl.DeviceIdType.MESH
COPIES = 128


def nt(a, b):
    return lax.dot_general(a, b, (((1,), (1,)), ((), ())), preferred_element_type=F32)


def nn(a, b):
    return lax.dot_general(a, b, (((1,), (0,)), ((), ())), preferred_element_type=F32)


def kernel(
    norm, cot_h, acts_h, pre_h, up_h, ups_h, down_h, dsc_h,
    gi_out, gu_out, gd_out,
    loc_s, loc_a, xs, xa, pre_r, act_t, wd, wu, da, dr, dpre,
    pd, td1, td2, fd, rd, farxd, nearxd, gotd, rawd, vd, faryd, nearyd, faryd2, nearyd2,
    pu, tu1, tu2, fu, ru, farxu, nearxu, gotu, rawu, vu, faryu, nearyu, faryu2, nearyu2,
    gi, farz, nearz, fz, rz,
    cot, acts, pre, up, ups, down, dsc,
    ssem, rsem, lsem,
):
    r, f, z = (lax.axis_index(n) for n in ("rep", "fs", "tp"))
    y = lax.div(f, 4)
    xl = lax.rem(lax.div(f, 2), 2)
    c = lax.rem(f, 2)
    x = r * 2 + xl
    oc, ox = 1 - c, 1 - xl

    def dev(dx=0, dy=0, dz=0, core=None):
        nx, ny, nz = (lax.rem(a + d + 4, 4) for a, d in ((x, dx), (y, dy), (z, dz)))
        core = c if core is None else core
        return {
            "rep": lax.div(nx, 2),
            "fs": ny * 4 + lax.rem(nx, 2) * 2 + core,
            "tp": nz,
        }

    def at(a, d):
        return lax.rem(a + d + 4, 4)

    barrier = pltpu.get_barrier_semaphore()
    peers = [dev(dz=d, core=k) for d in (1, -1) for k in (c, oc)]
    peers += [dev(dy=1), dev(dy=-1), dev(dx=1), dev(dx=-1), dev(dx=2), dev(core=oc)]
    for p in peers:
        pl.semaphore_signal(barrier, inc=1, device_id=p, device_id_type=MESH)

    loads = {}
    for i, (n, src, dst) in enumerate((
        ("dsc", dsc_h, dsc), ("cot", cot_h, cot), ("down", down_h, down), ("acts", acts_h, acts),
        ("up", up_h, up), ("pre", pre_h, pre), ("ups", ups_h, ups),
    )):
        loads[n] = pltpu.make_async_copy(src, dst, lsem.at[i])
        loads[n].start()
    started = []

    def send(src, dst, to):
        k = len(started)
        copy = pltpu.make_async_remote_copy(
            src_ref=src, dst_ref=dst, send_sem=ssem.at[k], recv_sem=rsem.at[k],
            device_id=to, device_id_type=MESH,
        )
        copy.start()
        started.append(copy)
        return copy

    def split(dst, v):
        for k in range(2):
            for j in range(2):
                lanes = slice(j * 256 + k * 128, j * 256 + k * 128 + 128)
                dst[k, :, j * 128:(j + 1) * 128] = v[:, lanes]

    loads["dsc"].wait()
    scale = dsc[:, pl.ds(pl.multiple_of(z * 512, 512), 512)]
    loads["cot"].wait()
    split(loc_s, (cot[...].astype(F32) * scale).astype(BF))
    xs[z, 0:256, :] = loc_s[c]
    loads["down"].wait()
    wd[y, xl] = down[...].astype(BF)
    loads["acts"].wait()
    split(loc_a, acts[...])
    xa[z, 0:256, :] = loc_a[c]
    loads["up"].wait()
    wu[y, xl] = up[...].astype(BF)
    loads["pre"].wait()
    loads["ups"].wait()
    pl.semaphore_wait(barrier, len(peers))

    own, other = pl.ds(0, 256), pl.ds(256, 256)

    def z_send(loc, full):
        def go(k, dz):
            part = own if k is c else other
            return send(loc.at[k], full.at[z, part, :], dev(dz=dz, core=k))

        return [go(c, 1), go(oc, -1), go(oc, 1), go(c, -1), go(oc, 0)]

    def z_forward(full, first):
        first[0].wait_recv()
        a = same(full.at[at(z, -1), own, :], dev(dz=1))
        first[1].wait_recv()
        b = same(full.at[at(z, 1), other, :], dev(dz=-1))
        return first[2:] + [a, b]

    def same(ref, to):
        return send(ref, ref, to)

    def wait_recv(copies):
        for k in copies:
            k.wait_recv()

    def add(a, b):
        return a.astype(F32) + b.astype(F32)

    def relu_sq(v):
        p = jnp.maximum(v.astype(F32), 0.0)
        return (p * p).astype(BF)

    def rows_of(ref, k, xx, lo, n):
        return ref.at[k, xx, pl.ds(lo, n), :]

    yn, yp, xn, xp, zn, zp = dev(dy=1), dev(dy=-1), dev(dx=1), dev(dx=-1), dev(dz=1), dev(dz=-1)

    def x_send(w, lo, n, k, h):
        return same(rows_of(w, k, xl, lo + h * n, n), xp if h else xn)

    class Ring:
        def __init__(self, view, me, far, near, nxt, prv):
            self.view, self.me, self.far, self.near = view, me, far, near
            self.nxt, self.prv = nxt, prv

        def start_far(self):
            k = at(self.me, 2)
            self.f = [
                send(self.view(k, 0), self.far.at[0], self.nxt),
                send(self.view(k, 1), self.far.at[1], self.prv),
            ]

        def start_near(self):
            self.n = [
                send(self.view(at(self.me, 1), 1), self.near.at[0, 1], self.nxt),
                send(self.view(at(self.me, -1), 0), self.near.at[1, 0], self.prv),
            ]

        def mid(self):
            for h, d, to in ((0, 1, self.nxt), (1, -1, self.prv)):
                self.f[h].wait_recv()
                v = self.view(at(self.me, d), h)
                v[...] = add(v[...], self.far[h]).astype(BF)
                self.n.append(send(v, self.near.at[h, h], to))

        def result(self):
            wait_recv(self.n)
            for h in range(2):
                v = self.view(self.me, h)
                yield h, add(v[...], self.near[0, h]) + self.near[1, h].astype(F32)

    class Grad:
        def __init__(self, p, t1, t2, fin, rr, farx, nearx, got, raw, vb, fary, neary, fary2, neary2):
            n = fin.shape[0] // 2
            self.p, self.t1, self.t2, self.fin, self.rr = p, t1, t2, fin, rr
            self.got, self.raw, self.vb = got, raw, vb
            self.x1 = Ring(
                lambda k, h: p.at[pl.ds(2 * h, 2), lax.rem(k, 2), 0, lax.div(k, 2)],
                x, farx, nearx, xn, xp,
            )
            self.y1 = Ring(lambda k, h: p.at[k, h, 1], y, fary, neary, yn, yp)
            self.y2 = Ring(
                lambda k, h: t1.at[k, pl.ds(h * n, n), :], y, fary2, neary2, yn, yp
            )
            self.n = n

        def start(self):
            self.y1.start_far()
            self.x1.start_far()
            self.y1.start_near()
            self.x1.start_near()

        def mid(self):
            self.y1.mid()
            self.x1.mid()

        def second_y(self):
            for h, v in self.x1.result():
                self.t1[2 * h:2 * h + 2] = v.astype(BF)
            self.y2.start_far()
            self.y2.start_near()

        def second_x(self):
            t2, got, raw = self.t2, self.got, self.raw
            for h, v in self.y1.result():
                t2[h] = v.astype(BF)
            self.c1 = [
                send(t2.at[xl, r], got.at[0], xn),
                send(t2.at[xl, 1 - r], got.at[1], xp),
            ]
            self.c2 = [
                send(t2.at[ox, 1 - mine], raw.at[0], xn),
                send(t2.at[ox, 1 - mine], raw.at[1], xp),
            ]

        def second_x_mid(self):
            wait_recv(self.c1)
            v = self.t2.at[ox, mine]
            v[...] = (add(self.got[0], self.got[1]) + v[...].astype(F32)).astype(BF)
            self.c2 += [send(v, self.vb.at[0], xn), send(v, self.vb.at[1], xp)]

        def store_second(self, out):
            wait_recv(self.c2)
            out[1, 1 - r] = add(self.vb[0], self.raw[1]) * norm
            out[1, r] = add(self.vb[1], self.raw[0]) * norm

        def share(self):
            for h, v in self.y2.result():
                self.fin[h * self.n:(h + 1) * self.n, :] = v.astype(BF)
            self.g = send(self.fin, self.rr, dev(dx=2))

        def store_first(self, out):
            out[0, r] = self.fin[...].astype(F32) * norm
            self.g.wait_recv()
            out[0, 1 - r] = self.rr[...].astype(F32) * norm

    mine = r * xl + (1 - r) * ox
    gd = Grad(pd, td1, td2, fd, rd, farxd, nearxd, gotd, rawd, vd, faryd, nearyd, faryd2, nearyd2)
    gu = Grad(pu, tu1, tu2, fu, ru, farxu, nearxu, gotu, rawu, vu, faryu, nearyu, faryu2, nearyu2)
    scope = jax.named_scope

    with scope("a_first_sends"):
        s1 = z_send(loc_s, xs)
        wd1 = [
            same(rows_of(wd, y, xl, 512 * h, 512), to)
            for h, to in ((0, yn), (1, yp), (1, yn), (0, yp))
        ]
        wdx = {d: [] for d in (0, 1, -1, 2)}
        wdx[0] = [x_send(wd, 0, 512, y, h) for h in range(2)]
        pre1 = send(pre, pre_r, dev(core=oc))
        wu_x = [x_send(wu, 64, 32, y, h) for h in range(2)]
    with scope("b_wd_first"):
        wd1[0].wait_recv()
        wd2 = [same(rows_of(wd, at(y, -1), xl, 0, 512), yn)]
        wdx[-1].append(x_send(wd, 0, 512, at(y, -1), 0))
        wd1[1].wait_recv()
        wd2.append(same(rows_of(wd, at(y, 1), xl, 512, 512), yp))
        wdx[1].append(x_send(wd, 0, 512, at(y, 1), 1))
    with scope("c_z_forward"):
        s2 = z_forward(xs, s1)
        a1 = z_send(loc_a, xa)
    with scope("d_wd_second"):
        wd1[2].wait_recv()
        wdx[-1].append(x_send(wd, 0, 512, at(y, -1), 1))
        wd1[3].wait_recv()
        wdx[1].append(x_send(wd, 0, 512, at(y, 1), 0))
        wuy = [same(rows_of(wu, y, xl, 0, 64), to) for to in (yn, yp)]
        wuo = [same(rows_of(wu, y, xl, 64, 64), to) for to in (yn, yp)]
        wuo2 = []
        for h in range(2):
            wu_x[h].wait_recv()
            piece = rows_of(wu, y, ox, 64 + 32 * h, 32)
            wuo2 += [same(piece, yn), same(piece, yp)]
    with scope("e_act"):
        act_t[:, 0:256] = relu_sq(pre[...]).T
        pre1.wait_recv()
        act_t[:, 256:512] = relu_sq(pre_r[...]).T
    with scope("f_wd_third"):
        for h in range(2):
            wd2[h].wait_recv()
            wdx[2].append(x_send(wd, 0, 512, at(y, 2), h))
        wux = [x_send(wu, 0, 32, y, h) for h in range(2)]
    with scope("g_scaled_wait"):
        wait_recv(s2)
    with scope("h_grad_down"):
        for k in range(4):
            part = nn(act_t[...], xs[k])
            for j in range(2):
                pd[k, j] = part[:, j * 128:(j + 1) * 128].astype(BF).reshape(2, 2, 256, 128)
        gd.y1.start_far()
        gd.x1.start_far()
        gd.x1.start_near()
    with scope("i_wu_second"):
        wuf = []
        for h, to, d in ((0, yn, -1), (1, yp, 1)):
            wuy[h].wait_recv()
            k = at(y, d)
            wuf.append(same(rows_of(wu, k, xl, 32 * h, 32), to))
            wux += [x_send(wu, 0, 32, k, 0), x_send(wu, 0, 32, k, 1)]
    with scope("j_acts_forward"):
        a2 = z_forward(xa, a1)
    dax = []
    for d in (0, 1, -1, 2):
        with scope("k_wd_wait"):
            wait_recv(wdx[d])
        with scope("l_d_act"):
            k = at(y, d)
            w = jnp.concatenate([wd[k, 0], wd[k, 1]], axis=1)
            for h in (0, 1):
                term = nt(xs[k, h * 256:(h + 1) * 256, :], w)
                da[h] = term if d == 0 else da[h] + term
                if d == 2:
                    dax.append(send(da.at[h], dr.at[1 - h], dev(core=oc)))
    with scope("m_wu_third"):
        wuo[0].wait_recv()
        wug = [same(rows_of(wu, at(y, -1), xl, 64, 64), yn)]
        for h in range(2):
            wuo2[2 * h + 1].wait_recv()
            wug.append(same(rows_of(wu, at(y, 1), ox, 64 + 32 * h, 32), yp))
        gd.y1.start_near()
    with scope("n_dpre"):
        for h in (1, 0):
            dax[1 - h].wait_recv()
            src = pre if h == 0 else pre_r
            pos = jnp.maximum(src[...].astype(F32), 0.0)
            dpre[h * 256:(h + 1) * 256, :] = (2.0 * pos * (da[h] + dr[h]) * ups[...]).astype(BF)
    with scope("o_acts_wait"):
        wait_recv(a2)
    with scope("p_grad_up"):
        for k in range(4):
            part = nn(xa[k].T, dpre[...])
            for j in range(2):
                pu[k, j] = part[j * 128:(j + 1) * 128, :].astype(BF).reshape(2, 2, 32, 1024)
    with scope("q_gd_mid"):
        for h in range(2):
            wuf[h].wait_recv()
            wux.append(x_send(wu, 0, 32, at(y, 2), h))
        gd.x1.mid()
        gd.y1.mid()
        gu.start()
    zr = Ring(lambda k, h: gi.at[k, pl.ds(256 * h, 256), :], z, farz, nearz, zn, zp)
    with scope("r_wu_wait"):
        wait_recv(wux)
        wait_recv(wuo[1:] + [wuo2[0], wuo2[2]] + wug)
    with scope("s_grad_in"):
        for d in (2, 1, -1, 0):
            k = at(z, d)
            gi[k] = nt(dpre[...], wu[k].reshape(256, 1024)).astype(BF)
            if d == 2:
                zr.start_far()
            if d == -1:
                zr.start_near()
    with scope("t_gd_second"):
        gd.second_y()
        gd.second_x()
    with scope("u_gu_mid"):
        gu.mid()
    with scope("v_z_mid"):
        zr.mid()
    with scope("w_gd_second_mid"):
        gd.y2.mid()
        gd.second_x_mid()
    with scope("y_gd_share"):
        gd.share()
    with scope("x_gu_second"):
        gu.second_y()
        gu.second_x()
    with scope("z_gi"):
        for h, v in zr.result():
            fz[h] = v.astype(BF)
        gx = send(fz.at[1], rz, dev(core=oc))
    with scope("za_gu_y2_mid"):
        gu.y2.mid()
    with scope("zb_gu_x2_mid"):
        gu.second_x_mid()
    with scope("zc_gi_out"):
        gx.wait_recv()
        for j in range(2):
            lanes = pl.ds(pl.multiple_of(j * 256 + c * 128, 128), 128)
            gi_out[:, lanes] = fz[0, :, j * 128:(j + 1) * 128]
            lanes = pl.ds(pl.multiple_of(j * 256 + oc * 128, 128), 128)
            gi_out[:, lanes] = rz[:, j * 128:(j + 1) * 128]
    with scope("zd_gu_share"):
        gu.share()
    with scope("ze_gd_out"):
        gd.store_first(gd_out)
        gd.store_second(gd_out)
    with scope("zf_gu_out"):
        gu.store_second(gu_out)
    with scope("zg_gu_out"):
        gu.store_first(gu_out)
    with scope("zh_drain"):
        for copy in started:
            copy.wait_send()


def body(acts, cotangent, pre_act, up_store, up_scale, down_store, down_scale):
    tokens = acts.shape[0] * lax.axis_size("fs") * lax.axis_size("rep")
    norm = 1.0 / math.sqrt(tokens)

    def vm(*shape, dtype=BF):
        return pltpu.VMEM(shape, dtype)

    def grad_bufs(n, m):
        return [
            vm(4, 2, 2, 2, n, m), vm(4, n, m), vm(2, 2, n, m), vm(n, m), vm(n, m),
            vm(2, 2, n, m), vm(2, 2, 2, n, m), vm(2, n, m), vm(2, n, m), vm(2, n, m),
            vm(2, 2, n, m), vm(2, 2, 2, n, m), vm(2, n // 2, m), vm(2, 2, n // 2, m),
        ]

    spec = pl.BlockSpec(memory_space=pltpu.VMEM)

    def call(*args):
        return kernel(norm, *args)

    gi, gu, gd = pl.pallas_call(
        call,
        name="ffn_backward",
        out_shape=(
            jax.ShapeDtypeStruct((256, 512), BF),
            jax.ShapeDtypeStruct((2, 2, 32, 1024), F32),
            jax.ShapeDtypeStruct((2, 2, 256, 128), F32),
        ),
        in_specs=[pl.BlockSpec(memory_space=pl.ANY)] * 7,
        out_specs=(spec,) * 3,
        scratch_shapes=[
            vm(2, 256, 256), vm(2, 256, 256), vm(4, 512, 256), vm(4, 512, 256),
            vm(256, 1024), vm(1024, 512), vm(4, 2, 1024, 128), vm(4, 2, 128, 1024),
            vm(2, 256, 1024, dtype=F32), vm(2, 256, 1024, dtype=F32), vm(512, 1024),
            *grad_bufs(256, 128),
            *grad_bufs(32, 1024),
            vm(4, 512, 256), vm(2, 256, 256), vm(2, 2, 256, 256), vm(2, 256, 256), vm(256, 256),
            vm(256, 512), vm(256, 512), vm(256, 1024), vm(128, 1024, dtype=F32),
            vm(1, 1024, dtype=F32), vm(1024, 128, dtype=F32), vm(1, 2048, dtype=F32),
            pltpu.SemaphoreType.DMA((COPIES,)),
            pltpu.SemaphoreType.DMA((COPIES,)),
            pltpu.SemaphoreType.DMA((7,)),
        ],
        compiler_params=pltpu.CompilerParams(
            collective_id=0, has_side_effects=True, vmem_limit_bytes=56 * 1024 * 1024
        ),
    )(
        cotangent, acts, pre_act, up_store, up_scale.reshape(1, -1),
        down_store, down_scale.reshape(1, -1),
    )
    return gi, gu.reshape(up_store.shape), gd.reshape(down_store.shape)


def solution(mesh):
    return jax.shard_map(
        body,
        mesh=mesh,
        in_specs=(
            P(("rep", "fs"), "tp"),
            P(("rep", "fs"), "tp"),
            P(("rep", "fs"), "tp"),
            P("fs", "tp"),
            P("tp"),
            P("tp", "fs"),
            P(),
        ),
        out_specs=(P(("rep", "fs"), "tp"), P("fs", "tp"), P("tp", "fs")),
        check_vma=False,
    )
```

```python
import math

import jax
import jax.numpy as jnp
from jax import lax
from jax.experimental import pallas as pl
from jax.experimental.pallas import tpu as pltpu
from jax.sharding import PartitionSpec as P

BF = jnp.bfloat16
F32 = jnp.float32
MESH = pl.DeviceIdType.MESH
RECVS = 57
SENT_ROWS = 52736


def nt(a, b):
    return lax.dot_general(a, b, (((1,), (1,)), ((), ())), preferred_element_type=F32)


def nn(a, b):
    return lax.dot_general(a, b, (((1,), (0,)), ((), ())), preferred_element_type=F32)


def kernel(
    norm, cot_h, acts_h, pre_h, up_h, ups_h, down_h, dsc_h,
    gi_out, gu_out, gd_out,
    loc_s, loc_a, xs, xa, pre_r, act_t, wd, wu, da, dr, dpre,
    pd, td1, td2, fd, rd, farxd, nearxd, gotd, rawd, vd, faryd, nearyd, faryd2, nearyd2,
    pu, tu1, tu2, fu, ru, farxu, nearxu, gotu, rawu, vu, faryu, nearyu, faryu2, nearyu2,
    gi, farz, nearz, fz, rz,
    cot, acts, pre, up, ups, down, dsc,
    sent, ssem, rsem, lsem,
):
    r, f, z = (lax.axis_index(n) for n in ("rep", "fs", "tp"))
    y = lax.div(f, 4)
    xl = lax.rem(lax.div(f, 2), 2)
    c = lax.rem(f, 2)
    x = r * 2 + xl
    oc, ox = 1 - c, 1 - xl

    def dev(dx=0, dy=0, dz=0, core=None):
        nx, ny, nz = (lax.rem(a + d + 4, 4) for a, d in ((x, dx), (y, dy), (z, dz)))
        core = c if core is None else core
        return {
            "rep": lax.div(nx, 2),
            "fs": ny * 4 + lax.rem(nx, 2) * 2 + core,
            "tp": nz,
        }

    def at(a, d):
        return lax.rem(a + d + 4, 4)

    barrier = pltpu.get_barrier_semaphore()
    peers = [dev(dz=d, core=k) for d in (1, -1) for k in (c, oc)]
    peers += [dev(dy=1), dev(dy=-1), dev(dx=1), dev(dx=-1), dev(dx=2), dev(core=oc)]
    for p in peers:
        pl.semaphore_signal(barrier, inc=1, device_id=p, device_id_type=MESH)

    loads = {}
    for i, (n, src, dst) in enumerate((
        ("dsc", dsc_h, dsc), ("cot", cot_h, cot), ("down", down_h, down), ("acts", acts_h, acts),
        ("up", up_h, up), ("pre", pre_h, pre), ("ups", ups_h, ups),
    )):
        loads[n] = pltpu.make_async_copy(src, dst, lsem.at[i])
        loads[n].start()
    started = []

    recvs = [0]

    def blank(rows):
        return sent.at[pl.ds(0, rows), :]

    def rows_in(ref):
        return math.prod(ref.shape) * jnp.dtype(ref.dtype).itemsize // 256

    class Group:
        def __init__(self):
            self.k, self.rows = recvs[0], 0
            recvs[0] += 1

        def wait_recv(self):
            d = blank(self.rows)
            pltpu.make_async_copy(d, d, rsem.at[self.k]).wait()

    def send(src, dst, to, group=None):
        group = group or Group()
        group.rows += rows_in(src)
        copy = pltpu.make_async_remote_copy(
            src_ref=src, dst_ref=dst, send_sem=ssem, recv_sem=rsem.at[group.k],
            device_id=to, device_id_type=MESH,
        )
        copy.start()
        started.append(rows_in(src))
        return group

    def split(dst, v):
        for k in range(2):
            for j in range(2):
                lanes = slice(j * 256 + k * 128, j * 256 + k * 128 + 128)
                dst[k, :, j * 128:(j + 1) * 128] = v[:, lanes]

    loads["dsc"].wait()
    scale = dsc[:, pl.ds(pl.multiple_of(z * 512, 512), 512)]
    loads["cot"].wait()
    split(loc_s, (cot[...].astype(F32) * scale).astype(BF))
    xs[z, 0:256, :] = loc_s[c]
    loads["down"].wait()
    wd[y, xl] = down[...].astype(BF)
    loads["acts"].wait()
    split(loc_a, acts[...])
    xa[z, 0:256, :] = loc_a[c]
    loads["up"].wait()
    wu[y, xl] = up[...].astype(BF)
    loads["pre"].wait()
    loads["ups"].wait()
    pl.semaphore_wait(barrier, len(peers))

    own, other = pl.ds(0, 256), pl.ds(256, 256)

    def same(ref, to, group=None):
        return send(ref, ref, to, group)

    def z_send(loc, full):
        rest = Group()

        def go(k, dz, group=None):
            part = own if k is c else other
            return send(loc.at[k], full.at[z, part, :], dev(dz=dz, core=k), group)

        first = [go(c, 1), go(oc, -1)]
        for k, dz in ((oc, 1), (c, -1), (oc, 0)):
            go(k, dz, rest)
        return first, rest

    def z_forward(full, sends):
        first, rest = sends
        first[0].wait_recv()
        same(full.at[at(z, -1), own, :], dev(dz=1), rest)
        first[1].wait_recv()
        same(full.at[at(z, 1), other, :], dev(dz=-1), rest)
        return rest

    def add(a, b):
        return a.astype(F32) + b.astype(F32)

    def relu_sq(v):
        p = jnp.maximum(v.astype(F32), 0.0)
        return (p * p).astype(BF)

    def rows_of(ref, k, xx, lo, n):
        return ref.at[k, xx, pl.ds(lo, n), :]

    yn, yp, xn, xp, zn, zp = dev(dy=1), dev(dy=-1), dev(dx=1), dev(dx=-1), dev(dz=1), dev(dz=-1)

    def x_send(w, lo, n, k, h, group=None):
        return same(rows_of(w, k, xl, lo + h * n, n), xp if h else xn, group)

    class Ring:
        def __init__(self, view, me, far, near, nxt, prv):
            self.view, self.me, self.far, self.near = view, me, far, near
            self.nxt, self.prv = nxt, prv

        def start_far(self):
            k = at(self.me, 2)
            self.f = [
                send(self.view(k, 0), self.far.at[0], self.nxt),
                send(self.view(k, 1), self.far.at[1], self.prv),
            ]

        def start_near(self):
            self.n = Group()
            send(self.view(at(self.me, 1), 1), self.near.at[0, 1], self.nxt, self.n)
            send(self.view(at(self.me, -1), 0), self.near.at[1, 0], self.prv, self.n)

        def mid(self):
            for h, d, to in ((0, 1, self.nxt), (1, -1, self.prv)):
                self.f[h].wait_recv()
                v = self.view(at(self.me, d), h)
                v[...] = add(v[...], self.far[h]).astype(BF)
                send(v, self.near.at[h, h], to, self.n)

        def result(self):
            self.n.wait_recv()
            for h in range(2):
                v = self.view(self.me, h)
                yield h, add(v[...], self.near[0, h]) + self.near[1, h].astype(F32)

    class Grad:
        def __init__(self, p, t1, t2, fin, rr, farx, nearx, got, raw, vb, fary, neary, fary2, neary2):
            n = fin.shape[0] // 2
            self.p, self.t1, self.t2, self.fin, self.rr = p, t1, t2, fin, rr
            self.got, self.raw, self.vb = got, raw, vb
            self.x1 = Ring(
                lambda k, h: p.at[pl.ds(2 * h, 2), lax.rem(k, 2), 0, lax.div(k, 2)],
                x, farx, nearx, xn, xp,
            )
            self.y1 = Ring(lambda k, h: p.at[k, h, 1], y, fary, neary, yn, yp)
            self.y2 = Ring(
                lambda k, h: t1.at[k, pl.ds(h * n, n), :], y, fary2, neary2, yn, yp
            )
            self.n = n

        def start(self):
            self.y1.start_far()
            self.x1.start_far()
            self.y1.start_near()
            self.x1.start_near()

        def mid(self):
            self.y1.mid()
            self.x1.mid()

        def second_y(self):
            for h, v in self.x1.result():
                self.t1[2 * h:2 * h + 2] = v.astype(BF)
            self.y2.start_far()
            self.y2.start_near()

        def second_x(self):
            t2, got, raw = self.t2, self.got, self.raw
            for h, v in self.y1.result():
                t2[h] = v.astype(BF)
            self.c1, self.c2 = Group(), Group()
            send(t2.at[xl, r], got.at[0], xn, self.c1)
            send(t2.at[xl, 1 - r], got.at[1], xp, self.c1)
            send(t2.at[ox, 1 - mine], raw.at[0], xn, self.c2)
            send(t2.at[ox, 1 - mine], raw.at[1], xp, self.c2)

        def second_x_mid(self):
            self.c1.wait_recv()
            v = self.t2.at[ox, mine]
            v[...] = (add(self.got[0], self.got[1]) + v[...].astype(F32)).astype(BF)
            send(v, self.vb.at[0], xn, self.c2)
            send(v, self.vb.at[1], xp, self.c2)

        def store_second(self, out):
            self.c2.wait_recv()
            out[1, 1 - r] = add(self.vb[0], self.raw[1]) * norm
            out[1, r] = add(self.vb[1], self.raw[0]) * norm

        def share(self):
            for h, v in self.y2.result():
                self.fin[h * self.n:(h + 1) * self.n, :] = v.astype(BF)
            self.g = send(self.fin, self.rr, dev(dx=2))

        def store_first(self, out):
            out[0, r] = self.fin[...].astype(F32) * norm
            self.g.wait_recv()
            out[0, 1 - r] = self.rr[...].astype(F32) * norm

    mine = r * xl + (1 - r) * ox
    gd = Grad(pd, td1, td2, fd, rd, farxd, nearxd, gotd, rawd, vd, faryd, nearyd, faryd2, nearyd2)
    gu = Grad(pu, tu1, tu2, fu, ru, farxu, nearxu, gotu, rawu, vu, faryu, nearyu, faryu2, nearyu2)
    scope = jax.named_scope

    with scope("a_first_sends"):
        s1 = z_send(loc_s, xs)
        wd1 = [
            same(rows_of(wd, y, xl, 512 * h, 512), to)
            for h, to in ((0, yn), (1, yp), (1, yn), (0, yp))
        ]
        wdx = {d: Group() for d in (0, 1, -1, 2)}
        for h in range(2):
            x_send(wd, 0, 512, y, h, wdx[0])
        pre1 = send(pre, pre_r, dev(core=oc))
        wu_x = [x_send(wu, 64, 32, y, h) for h in range(2)]
    with scope("b_wd_first"):
        wd1[0].wait_recv()
        wd2 = [same(rows_of(wd, at(y, -1), xl, 0, 512), yn)]
        x_send(wd, 0, 512, at(y, -1), 0, wdx[-1])
        wd1[1].wait_recv()
        wd2.append(same(rows_of(wd, at(y, 1), xl, 512, 512), yp))
        x_send(wd, 0, 512, at(y, 1), 1, wdx[1])
    with scope("c_z_forward"):
        s2 = z_forward(xs, s1)
        a1 = z_send(loc_a, xa)
    with scope("d_wd_second"):
        wd1[2].wait_recv()
        x_send(wd, 0, 512, at(y, -1), 1, wdx[-1])
        wd1[3].wait_recv()
        x_send(wd, 0, 512, at(y, 1), 0, wdx[1])
        wuy = [same(rows_of(wu, y, xl, 0, 64), to) for to in (yn, yp)]
        wux = Group()
        wuo = same(rows_of(wu, y, xl, 64, 64), yn)
        same(rows_of(wu, y, xl, 64, 64), yp, wux)
        wuo2 = []
        for h in range(2):
            wu_x[h].wait_recv()
            piece = rows_of(wu, y, ox, 64 + 32 * h, 32)
            same(piece, yn, wux)
            wuo2.append(same(piece, yp))
    with scope("e_act"):
        act_t[:, 0:256] = relu_sq(pre[...]).T
        pre1.wait_recv()
        act_t[:, 256:512] = relu_sq(pre_r[...]).T
    with scope("f_wd_third"):
        for h in range(2):
            wd2[h].wait_recv()
            x_send(wd, 0, 512, at(y, 2), h, wdx[2])
        for h in range(2):
            x_send(wu, 0, 32, y, h, wux)
    with scope("g_scaled_wait"):
        s2.wait_recv()
    with scope("h_grad_down"):
        for k in range(4):
            part = nn(act_t[...], xs[k])
            for j in range(2):
                pd[k, j] = part[:, j * 128:(j + 1) * 128].astype(BF).reshape(2, 2, 256, 128)
        gd.y1.start_far()
        gd.x1.start_far()
        gd.x1.start_near()
    with scope("i_wu_second"):
        wuf = []
        for h, to, d in ((0, yn, -1), (1, yp, 1)):
            wuy[h].wait_recv()
            k = at(y, d)
            wuf.append(same(rows_of(wu, k, xl, 32 * h, 32), to))
            x_send(wu, 0, 32, k, 0, wux)
            x_send(wu, 0, 32, k, 1, wux)
    with scope("j_acts_forward"):
        a2 = z_forward(xa, a1)
    dax = []
    for d in (0, 1, -1, 2):
        with scope("k_wd_wait"):
            wdx[d].wait_recv()
        with scope("l_d_act"):
            k = at(y, d)
            w = jnp.concatenate([wd[k, 0], wd[k, 1]], axis=1)
            for h in (0, 1):
                term = nt(xs[k, h * 256:(h + 1) * 256, :], w)
                da[h] = term if d == 0 else da[h] + term
                if d == 2:
                    dax.append(send(da.at[h], dr.at[1 - h], dev(core=oc)))
    with scope("m_wu_third"):
        wuo.wait_recv()
        same(rows_of(wu, at(y, -1), xl, 64, 64), yn, wux)
        for h in range(2):
            wuo2[h].wait_recv()
            same(rows_of(wu, at(y, 1), ox, 64 + 32 * h, 32), yp, wux)
        gd.y1.start_near()
    with scope("n_dpre"):
        for h in (1, 0):
            dax[1 - h].wait_recv()
            src = pre if h == 0 else pre_r
            pos = jnp.maximum(src[...].astype(F32), 0.0)
            dpre[h * 256:(h + 1) * 256, :] = (2.0 * pos * (da[h] + dr[h]) * ups[...]).astype(BF)
    with scope("o_acts_wait"):
        a2.wait_recv()
    with scope("p_grad_up"):
        for k in range(4):
            part = nn(xa[k].T, dpre[...])
            for j in range(2):
                pu[k, j] = part[j * 128:(j + 1) * 128, :].astype(BF).reshape(2, 2, 32, 1024)
    with scope("q_gd_mid"):
        for h in range(2):
            wuf[h].wait_recv()
            x_send(wu, 0, 32, at(y, 2), h, wux)
        gd.x1.mid()
        gd.y1.mid()
        gu.start()
    zr = Ring(lambda k, h: gi.at[k, pl.ds(256 * h, 256), :], z, farz, nearz, zn, zp)
    with scope("r_wu_wait"):
        wux.wait_recv()
    with scope("s_grad_in"):
        for d in (2, 1, -1, 0):
            k = at(z, d)
            gi[k] = nt(dpre[...], wu[k].reshape(256, 1024)).astype(BF)
            if d == 2:
                zr.start_far()
            if d == -1:
                zr.start_near()
    with scope("t_gd_second"):
        gd.second_y()
        gd.second_x()
    with scope("u_gu_mid"):
        gu.mid()
    with scope("v_z_mid"):
        zr.mid()
    with scope("w_gd_second_mid"):
        gd.y2.mid()
        gd.second_x_mid()
    with scope("x_gu_second_x"):
        gu.second_x()
    with scope("x_gu_second_y"):
        gu.second_y()
    with scope("y_gd_share"):
        gd.share()
    with scope("z_gi"):
        for h, v in zr.result():
            fz[h] = v.astype(BF)
        gx = send(fz.at[1], rz, dev(core=oc))
    with scope("za_gu_y2_mid"):
        gu.y2.mid()
    with scope("zb_gu_x2_mid"):
        gu.second_x_mid()
    with scope("zc_gi_out"):
        gx.wait_recv()
        for j in range(2):
            lanes = pl.ds(pl.multiple_of(j * 256 + c * 128, 128), 128)
            gi_out[:, lanes] = fz[0, :, j * 128:(j + 1) * 128]
            lanes = pl.ds(pl.multiple_of(j * 256 + oc * 128, 128), 128)
            gi_out[:, lanes] = rz[:, j * 128:(j + 1) * 128]
    with scope("zd_gu_share"):
        gu.share()
    with scope("ze_gd_out"):
        gd.store_first(gd_out)
        gd.store_second(gd_out)
    with scope("zf_gu_out"):
        gu.store_second(gu_out)
    with scope("zg_gu_out"):
        gu.store_first(gu_out)
    with scope("zh_drain"):
        assert recvs[0] == RECVS and sum(started) == SENT_ROWS, (recvs, sum(started))
        pltpu.make_async_copy(sent, sent, ssem).wait()


def body(acts, cotangent, pre_act, up_store, up_scale, down_store, down_scale):
    tokens = acts.shape[0] * lax.axis_size("fs") * lax.axis_size("rep")
    norm = 1.0 / math.sqrt(tokens)

    def vm(*shape, dtype=BF):
        return pltpu.VMEM(shape, dtype)

    def grad_bufs(n, m):
        return [
            vm(4, 2, 2, 2, n, m), vm(4, n, m), vm(2, 2, n, m), vm(n, m), vm(n, m),
            vm(2, 2, n, m), vm(2, 2, 2, n, m), vm(2, n, m), vm(2, n, m), vm(2, n, m),
            vm(2, 2, n, m), vm(2, 2, 2, n, m), vm(2, n // 2, m), vm(2, 2, n // 2, m),
        ]

    spec = pl.BlockSpec(memory_space=pltpu.VMEM)

    def call(*args):
        return kernel(norm, *args)

    gi, gu, gd = pl.pallas_call(
        call,
        name="ffn_backward",
        out_shape=(
            pltpu.VMEM((256, 512), BF),
            pltpu.VMEM((2, 2, 32, 1024), F32),
            pltpu.VMEM((2, 2, 256, 128), F32),
        ),
        in_specs=[pl.BlockSpec(memory_space=pl.ANY)] * 7,
        out_specs=(spec,) * 3,
        scratch_shapes=[
            vm(2, 256, 256), vm(2, 256, 256), vm(4, 512, 256), vm(4, 512, 256),
            vm(256, 1024), vm(1024, 512), vm(4, 2, 1024, 128), vm(4, 2, 128, 1024),
            vm(2, 256, 1024, dtype=F32), vm(2, 256, 1024, dtype=F32), vm(512, 1024),
            *grad_bufs(256, 128),
            *grad_bufs(32, 1024),
            vm(4, 512, 256), vm(2, 256, 256), vm(2, 2, 256, 256), vm(2, 256, 256), vm(256, 256),
            vm(256, 512), vm(256, 512), vm(256, 1024), vm(128, 1024, dtype=F32),
            vm(1, 1024, dtype=F32), vm(1024, 128, dtype=F32), vm(1, 2048, dtype=F32),
            vm(SENT_ROWS, 128),
            pltpu.SemaphoreType.DMA,
            pltpu.SemaphoreType.DMA((RECVS,)),
            pltpu.SemaphoreType.DMA((7,)),
        ],
        compiler_params=pltpu.CompilerParams(
            collective_id=0, has_side_effects=True, vmem_limit_bytes=56 * 1024 * 1024
        ),
    )(
        cotangent, acts, pre_act, up_store, up_scale.reshape(1, -1),
        down_store, down_scale.reshape(1, -1),
    )
    return gi, gu.reshape(up_store.shape), gd.reshape(down_store.shape)


def solution(mesh):
    return jax.shard_map(
        body,
        mesh=mesh,
        in_specs=(
            P(("rep", "fs"), "tp"),
            P(("rep", "fs"), "tp"),
            P(("rep", "fs"), "tp"),
            P("fs", "tp"),
            P("tp"),
            P("tp", "fs"),
            P(),
        ),
        out_specs=(P(("rep", "fs"), "tp"), P("fs", "tp"), P("tp", "fs")),
        check_vma=False,
    )
```

```python
import math

import jax
import jax.numpy as jnp
from jax import lax
from jax.experimental import pallas as pl
from jax.experimental.pallas import tpu as pltpu
from jax.sharding import PartitionSpec as P

BF = jnp.bfloat16
F32 = jnp.float32
MESH = pl.DeviceIdType.MESH
RECVS = 57
Y_FIRST = 64
SENT_ROWS = 52736


def nt(a, b):
    return lax.dot_general(a, b, (((1,), (1,)), ((), ())), preferred_element_type=F32)


def nn(a, b):
    return lax.dot_general(a, b, (((1,), (0,)), ((), ())), preferred_element_type=F32)


def kernel(
    norm, cot_h, acts_h, pre_h, up_h, ups_h, down_h, dsc_h,
    gi_out, gu_out, gd_out,
    loc_s, loc_a, xs, xa, pre_r, act_t, wd, wu, da, dr, dpre,
    pd, td1, td2, fd, rd, farxd, nearxd, gotd, rawd, vd, faryd, nearyd, faryd2, nearyd2,
    pu, tu1, tu2, fu, ru, farxu, nearxu, gotu, rawu, vu, faryu, nearyu, faryu2, nearyu2,
    gi, farz, nearz, fz, rz,
    cot, acts, pre, up, ups, down, dsc,
    sent, ssem, rsem, lsem,
):
    r, f, z = (lax.axis_index(n) for n in ("rep", "fs", "tp"))
    y = lax.div(f, 4)
    xl = lax.rem(lax.div(f, 2), 2)
    c = lax.rem(f, 2)
    x = r * 2 + xl
    oc, ox = 1 - c, 1 - xl

    def dev(dx=0, dy=0, dz=0, core=None):
        nx, ny, nz = (lax.rem(a + d + 4, 4) for a, d in ((x, dx), (y, dy), (z, dz)))
        core = c if core is None else core
        return {
            "rep": lax.div(nx, 2),
            "fs": ny * 4 + lax.rem(nx, 2) * 2 + core,
            "tp": nz,
        }

    def at(a, d):
        return lax.rem(a + d + 4, 4)

    barrier = pltpu.get_barrier_semaphore()
    peers = [dev(dz=d, core=k) for d in (1, -1) for k in (c, oc)]
    peers += [dev(dy=1), dev(dy=-1), dev(dx=1), dev(dx=-1), dev(dx=2), dev(core=oc)]
    for p in peers:
        pl.semaphore_signal(barrier, inc=1, device_id=p, device_id_type=MESH)

    loads = {}
    for i, (n, src, dst) in enumerate((
        ("dsc", dsc_h, dsc), ("cot", cot_h, cot), ("down", down_h, down), ("acts", acts_h, acts),
        ("up", up_h, up), ("pre", pre_h, pre), ("ups", ups_h, ups),
    )):
        loads[n] = pltpu.make_async_copy(src, dst, lsem.at[i])
        loads[n].start()
    started = []

    recvs = [0]

    def blank(rows):
        return sent.at[pl.ds(0, rows), :]

    def rows_in(ref):
        return math.prod(ref.shape) * jnp.dtype(ref.dtype).itemsize // 256

    class Group:
        def __init__(self):
            self.k, self.rows = recvs[0], 0
            recvs[0] += 1

        def wait_recv(self):
            d = blank(self.rows)
            pltpu.make_async_copy(d, d, rsem.at[self.k]).wait()

    def send(src, dst, to, group=None):
        group = group or Group()
        group.rows += rows_in(src)
        copy = pltpu.make_async_remote_copy(
            src_ref=src, dst_ref=dst, send_sem=ssem, recv_sem=rsem.at[group.k],
            device_id=to, device_id_type=MESH,
        )
        copy.start()
        started.append(rows_in(src))
        return group

    def split(dst, v):
        for k in range(2):
            for j in range(2):
                lanes = slice(j * 256 + k * 128, j * 256 + k * 128 + 128)
                dst[k, :, j * 128:(j + 1) * 128] = v[:, lanes]

    loads["dsc"].wait()
    scale = dsc[:, pl.ds(pl.multiple_of(z * 512, 512), 512)]
    loads["cot"].wait()
    split(loc_s, (cot[...].astype(F32) * scale).astype(BF))
    xs[z, 0:256, :] = loc_s[c]
    loads["down"].wait()
    wd[y, xl] = down[...].astype(BF)
    loads["acts"].wait()
    split(loc_a, acts[...])
    xa[z, 0:256, :] = loc_a[c]
    loads["up"].wait()
    wu[y, xl] = up[...].astype(BF)
    loads["pre"].wait()
    loads["ups"].wait()
    pl.semaphore_wait(barrier, len(peers))

    own, other = pl.ds(0, 256), pl.ds(256, 256)

    def same(ref, to, group=None):
        return send(ref, ref, to, group)

    def z_send(loc, full):
        rest = Group()

        def go(k, dz, group=None):
            part = own if k is c else other
            return send(loc.at[k], full.at[z, part, :], dev(dz=dz, core=k), group)

        first = [go(c, 1), go(oc, -1)]
        for k, dz in ((oc, 1), (c, -1), (oc, 0)):
            go(k, dz, rest)
        return first, rest

    def z_forward(full, sends):
        first, rest = sends
        first[0].wait_recv()
        same(full.at[at(z, -1), own, :], dev(dz=1), rest)
        first[1].wait_recv()
        same(full.at[at(z, 1), other, :], dev(dz=-1), rest)
        return rest

    def add(a, b):
        return a.astype(F32) + b.astype(F32)

    def relu_sq(v):
        p = jnp.maximum(v.astype(F32), 0.0)
        return (p * p).astype(BF)

    def rows_of(ref, k, xx, lo, n):
        return ref.at[k, xx, pl.ds(lo, n), :]

    yn, yp, xn, xp, zn, zp = dev(dy=1), dev(dy=-1), dev(dx=1), dev(dx=-1), dev(dz=1), dev(dz=-1)

    def x_send(w, lo, n, k, h, group=None):
        return same(rows_of(w, k, xl, lo + h * n, n), xp if h else xn, group)

    class Ring:
        def __init__(self, view, me, far, near, nxt, prv):
            self.view, self.me, self.far, self.near = view, me, far, near
            self.nxt, self.prv = nxt, prv

        def start_far(self):
            k = at(self.me, 2)
            self.f = [
                send(self.view(k, 0), self.far.at[0], self.nxt),
                send(self.view(k, 1), self.far.at[1], self.prv),
            ]

        def start_near(self):
            self.n = Group()
            send(self.view(at(self.me, 1), 1), self.near.at[0, 1], self.nxt, self.n)
            send(self.view(at(self.me, -1), 0), self.near.at[1, 0], self.prv, self.n)

        def mid(self):
            for h, d, to in ((0, 1, self.nxt), (1, -1, self.prv)):
                self.f[h].wait_recv()
                v = self.view(at(self.me, d), h)
                v[...] = add(v[...], self.far[h]).astype(BF)
                send(v, self.near.at[h, h], to, self.n)

        def result(self):
            self.n.wait_recv()
            for h in range(2):
                v = self.view(self.me, h)
                yield h, add(v[...], self.near[0, h]) + self.near[1, h].astype(F32)

    class Grad:
        def __init__(self, p, t1, t2, fin, rr, farx, nearx, got, raw, vb, fary, neary, fary2, neary2):
            n = fin.shape[0] // 2
            self.p, self.t1, self.t2, self.fin, self.rr = p, t1, t2, fin, rr
            self.got, self.raw, self.vb = got, raw, vb
            self.x1 = Ring(
                lambda k, h: p.at[pl.ds(2 * h, 2), lax.rem(k, 2), 0, lax.div(k, 2)],
                x, farx, nearx, xn, xp,
            )
            self.y1 = Ring(lambda k, h: p.at[k, h, 1], y, fary, neary, yn, yp)
            self.y2 = Ring(
                lambda k, h: t1.at[k, pl.ds(h * n, n), :], y, fary2, neary2, yn, yp
            )
            self.n = n

        def start(self):
            self.y1.start_far()
            self.x1.start_far()
            self.y1.start_near()
            self.x1.start_near()

        def mid(self):
            self.y1.mid()
            self.x1.mid()

        def second_y(self):
            for h, v in self.x1.result():
                self.t1[2 * h:2 * h + 2] = v.astype(BF)
            self.y2.start_far()
            self.y2.start_near()

        def second_x(self):
            t2, got, raw = self.t2, self.got, self.raw
            for h, v in self.y1.result():
                t2[h] = v.astype(BF)
            self.c1, self.c2 = Group(), Group()
            send(t2.at[xl, r], got.at[0], xn, self.c1)
            send(t2.at[xl, 1 - r], got.at[1], xp, self.c1)
            send(t2.at[ox, 1 - mine], raw.at[0], xn, self.c2)
            send(t2.at[ox, 1 - mine], raw.at[1], xp, self.c2)

        def second_x_mid(self):
            self.c1.wait_recv()
            v = self.t2.at[ox, mine]
            v[...] = (add(self.got[0], self.got[1]) + v[...].astype(F32)).astype(BF)
            send(v, self.vb.at[0], xn, self.c2)
            send(v, self.vb.at[1], xp, self.c2)

        def store_second(self, out):
            self.c2.wait_recv()
            out[1, 1 - r] = add(self.vb[0], self.raw[1]) * norm
            out[1, r] = add(self.vb[1], self.raw[0]) * norm

        def share(self):
            for h, v in self.y2.result():
                self.fin[h * self.n:(h + 1) * self.n, :] = v.astype(BF)
            self.g = send(self.fin, self.rr, dev(dx=2))

        def store_first(self, out):
            out[0, r] = self.fin[...].astype(F32) * norm
            self.g.wait_recv()
            out[0, 1 - r] = self.rr[...].astype(F32) * norm

    mine = r * xl + (1 - r) * ox
    gd = Grad(pd, td1, td2, fd, rd, farxd, nearxd, gotd, rawd, vd, faryd, nearyd, faryd2, nearyd2)
    gu = Grad(pu, tu1, tu2, fu, ru, farxu, nearxu, gotu, rawu, vu, faryu, nearyu, faryu2, nearyu2)
    scope = jax.named_scope

    with scope("a_first_sends"):
        s1 = z_send(loc_s, xs)
        wd1 = [
            same(rows_of(wd, y, xl, 512 * h, 512), to)
            for h, to in ((0, yn), (1, yp), (1, yn), (0, yp))
        ]
        wdx = {d: Group() for d in (0, 1, -1, 2)}
        for h in range(2):
            x_send(wd, 0, 512, y, h, wdx[0])
        pre1 = send(pre, pre_r, dev(core=oc))
        ya, yh = Y_FIRST, Y_FIRST // 2
        xr, xh = 128 - ya, (128 - ya) // 2
        wu_x = [x_send(wu, ya, xh, y, h) for h in range(2)]
        wux = Group()
        for h in range(2):
            x_send(wu, 0, yh, y, h, wux)
    with scope("b_wd_first"):
        wd1[0].wait_recv()
        wd2 = [same(rows_of(wd, at(y, -1), xl, 0, 512), yn)]
        x_send(wd, 0, 512, at(y, -1), 0, wdx[-1])
        wd1[1].wait_recv()
        wd2.append(same(rows_of(wd, at(y, 1), xl, 512, 512), yp))
        x_send(wd, 0, 512, at(y, 1), 1, wdx[1])
    with scope("c_z_forward"):
        s2 = z_forward(xs, s1)
        a1 = z_send(loc_a, xa)
    with scope("d_wd_second"):
        wd1[2].wait_recv()
        x_send(wd, 0, 512, at(y, -1), 1, wdx[-1])
        wd1[3].wait_recv()
        x_send(wd, 0, 512, at(y, 1), 0, wdx[1])
        wuy = [same(rows_of(wu, y, xl, 0, ya), to) for to in (yn, yp)]
        wuo = same(rows_of(wu, y, xl, ya, xr), yn)
        same(rows_of(wu, y, xl, ya, xr), yp, wux)
        wuo2 = []
        for h in range(2):
            wu_x[h].wait_recv()
            piece = rows_of(wu, y, ox, ya + xh * h, xh)
            same(piece, yn, wux)
            wuo2.append(same(piece, yp))
    with scope("e_act"):
        act_t[:, 0:256] = relu_sq(pre[...]).T
        pre1.wait_recv()
        act_t[:, 256:512] = relu_sq(pre_r[...]).T
    with scope("f_wd_third"):
        for h in range(2):
            wd2[h].wait_recv()
            x_send(wd, 0, 512, at(y, 2), h, wdx[2])
    with scope("g_scaled_wait"):
        s2.wait_recv()
    with scope("h_grad_down"):
        for k in range(4):
            part = nn(act_t[...], xs[k])
            for j in range(2):
                pd[k, j] = part[:, j * 128:(j + 1) * 128].astype(BF).reshape(2, 2, 256, 128)
        gd.y1.start_far()
        gd.x1.start_far()
        gd.x1.start_near()
    with scope("i_wu_second"):
        wuf = []
        for h, to, d in ((0, yn, -1), (1, yp, 1)):
            wuy[h].wait_recv()
            k = at(y, d)
            wuf.append(same(rows_of(wu, k, xl, yh * h, yh), to))
            x_send(wu, 0, yh, k, 0, wux)
            x_send(wu, 0, yh, k, 1, wux)
    with scope("j_acts_forward"):
        a2 = z_forward(xa, a1)
    dax = []
    for d in (0, 1, -1, 2):
        with scope("k_wd_wait"):
            wdx[d].wait_recv()
        with scope("l_d_act"):
            k = at(y, d)
            w = jnp.concatenate([wd[k, 0], wd[k, 1]], axis=1)
            for h in (0, 1):
                term = nt(xs[k, h * 256:(h + 1) * 256, :], w)
                da[h] = term if d == 0 else da[h] + term
                if d == 2:
                    dax.append(send(da.at[h], dr.at[1 - h], dev(core=oc)))
    with scope("m_wu_third"):
        wuo.wait_recv()
        same(rows_of(wu, at(y, -1), xl, ya, xr), yn, wux)
        for h in range(2):
            wuo2[h].wait_recv()
            same(rows_of(wu, at(y, 1), ox, ya + xh * h, xh), yp, wux)
        gd.y1.start_near()
    with scope("n_dpre"):
        for h in (1, 0):
            dax[1 - h].wait_recv()
            src = pre if h == 0 else pre_r
            pos = jnp.maximum(src[...].astype(F32), 0.0)
            dpre[h * 256:(h + 1) * 256, :] = (2.0 * pos * (da[h] + dr[h]) * ups[...]).astype(BF)
    with scope("o_acts_wait"):
        a2.wait_recv()
    with scope("p_grad_up"):
        for k in range(4):
            part = nn(xa[k].T, dpre[...])
            for j in range(2):
                pu[k, j] = part[j * 128:(j + 1) * 128, :].astype(BF).reshape(2, 2, 32, 1024)
    with scope("q_gd_mid"):
        for h in range(2):
            wuf[h].wait_recv()
            x_send(wu, 0, yh, at(y, 2), h, wux)
        gd.x1.mid()
        gd.y1.mid()
        gu.start()
    zr = Ring(lambda k, h: gi.at[k, pl.ds(256 * h, 256), :], z, farz, nearz, zn, zp)
    with scope("r_wu_wait"):
        wux.wait_recv()
    with scope("s_grad_in"):
        for d in (2, 1, -1, 0):
            k = at(z, d)
            gi[k] = nt(dpre[...], wu[k].reshape(256, 1024)).astype(BF)
            if d == 2:
                zr.start_far()
            if d == -1:
                zr.start_near()
    with scope("u_gu_x1_mid"):
        gu.x1.mid()
    with scope("u_z_mid"):
        zr.mid()
    with scope("u_gu_y1_mid"):
        gu.y1.mid()
    with scope("t_gd_second"):
        gd.second_y()
        gd.second_x()
    with scope("w_gu_second_y"):
        gu.second_y()
    with scope("v_gd_x2_mid"):
        gd.second_x_mid()
    with scope("y_gu_second_x"):
        gu.second_x()
    with scope("v_gd_y2_mid"):
        gd.y2.mid()
    with scope("x_gi"):
        for h, v in zr.result():
            fz[h] = v.astype(BF)
        gx = send(fz.at[1], rz, dev(core=oc))
    with scope("za_gu_y2_mid"):
        gu.y2.mid()
    with scope("zb_gu_x2_mid"):
        gu.second_x_mid()
    with scope("zd_gu_share"):
        gu.share()
    with scope("z_gd_share"):
        gd.share()
    with scope("zc_gi_out"):
        gx.wait_recv()
        for j in range(2):
            lanes = pl.ds(pl.multiple_of(j * 256 + c * 128, 128), 128)
            gi_out[:, lanes] = fz[0, :, j * 128:(j + 1) * 128]
            lanes = pl.ds(pl.multiple_of(j * 256 + oc * 128, 128), 128)
            gi_out[:, lanes] = rz[:, j * 128:(j + 1) * 128]
    with scope("ze_gd_out"):
        gd.store_first(gd_out)
        gd.store_second(gd_out)
    with scope("zf_gu_out"):
        gu.store_second(gu_out)
    with scope("zg_gu_out"):
        gu.store_first(gu_out)
    with scope("zh_drain"):
        assert recvs[0] == RECVS and sum(started) == SENT_ROWS, (recvs, sum(started))
        pltpu.make_async_copy(sent, sent, ssem).wait()


def write_out(a, b, c, x, y, z, sems):
    copies = [
        pltpu.make_async_copy(v, w, sems.at[i])
        for i, (v, w) in enumerate(((a, x), (b, y), (c, z)))
    ]
    for k in copies:
        k.start()
    for k in copies:
        k.wait()


def body(acts, cotangent, pre_act, up_store, up_scale, down_store, down_scale):
    tokens = acts.shape[0] * lax.axis_size("fs") * lax.axis_size("rep")
    norm = 1.0 / math.sqrt(tokens)

    def vm(*shape, dtype=BF):
        return pltpu.VMEM(shape, dtype)

    def grad_bufs(n, m):
        return [
            vm(4, 2, 2, 2, n, m), vm(4, n, m), vm(2, 2, n, m), vm(n, m), vm(n, m),
            vm(2, 2, n, m), vm(2, 2, 2, n, m), vm(2, n, m), vm(2, n, m), vm(2, n, m),
            vm(2, 2, n, m), vm(2, 2, 2, n, m), vm(2, n // 2, m), vm(2, 2, n // 2, m),
        ]

    spec = pl.BlockSpec(memory_space=pltpu.VMEM)

    def call(*args):
        return kernel(norm, *args)

    gi, gu, gd = pl.pallas_call(
        call,
        name="ffn_backward",
        out_shape=(
            pltpu.VMEM((256, 512), BF),
            pltpu.VMEM((2, 2, 32, 1024), F32),
            pltpu.VMEM((2, 2, 256, 128), F32),
        ),
        in_specs=[pl.BlockSpec(memory_space=pl.ANY)] * 7,
        out_specs=(spec,) * 3,
        scratch_shapes=[
            vm(2, 256, 256), vm(2, 256, 256), vm(4, 512, 256), vm(4, 512, 256),
            vm(256, 1024), vm(1024, 512), vm(4, 2, 1024, 128), vm(4, 2, 128, 1024),
            vm(2, 256, 1024, dtype=F32), vm(2, 256, 1024, dtype=F32), vm(512, 1024),
            *grad_bufs(256, 128),
            *grad_bufs(32, 1024),
            vm(4, 512, 256), vm(2, 256, 256), vm(2, 2, 256, 256), vm(2, 256, 256), vm(256, 256),
            vm(256, 512), vm(256, 512), vm(256, 1024), vm(128, 1024, dtype=F32),
            vm(1, 1024, dtype=F32), vm(1024, 128, dtype=F32), vm(1, 2048, dtype=F32),
            vm(SENT_ROWS, 128),
            pltpu.SemaphoreType.DMA,
            pltpu.SemaphoreType.DMA((RECVS,)),
            pltpu.SemaphoreType.DMA((7,)),
        ],
        compiler_params=pltpu.CompilerParams(
            collective_id=0, has_side_effects=True, vmem_limit_bytes=56 * 1024 * 1024
        ),
    )(
        cotangent, acts, pre_act, up_store, up_scale.reshape(1, -1),
        down_store, down_scale.reshape(1, -1),
    )
    outs = [pltpu.with_memory_space_constraint(v, pltpu.VMEM) for v in (gi, gu, gd)]
    gi, gu, gd = pl.pallas_call(
        write_out,
        name="write_out",
        out_shape=tuple(jax.ShapeDtypeStruct(v.shape, v.dtype) for v in outs),
        in_specs=[spec] * 3,
        out_specs=(pl.BlockSpec(memory_space=pl.ANY),) * 3,
        scratch_shapes=[pltpu.SemaphoreType.DMA((3,))],
    )(*outs)
    return gi, gu.reshape(up_store.shape), gd.reshape(down_store.shape)


def solution(mesh):
    return jax.shard_map(
        body,
        mesh=mesh,
        in_specs=(
            P(("rep", "fs"), "tp"),
            P(("rep", "fs"), "tp"),
            P(("rep", "fs"), "tp"),
            P("fs", "tp"),
            P("tp"),
            P("tp", "fs"),
            P(),
        ),
        out_specs=(P(("rep", "fs"), "tp"), P("fs", "tp"), P("tp", "fs")),
        check_vma=False,
    )
```

```python
import math

import jax
import jax.numpy as jnp
from jax import lax
from jax.experimental import pallas as pl
from jax.experimental.pallas import tpu as pltpu
from jax.sharding import PartitionSpec as P

BF = jnp.bfloat16
F32 = jnp.float32
MESH = pl.DeviceIdType.MESH
RECVS = 69
Y_FIRST = 64
SENT_ROWS = 52736


def nt(a, b):
    return lax.dot_general(a, b, (((1,), (1,)), ((), ())), preferred_element_type=F32)


def nn(a, b):
    return lax.dot_general(a, b, (((1,), (0,)), ((), ())), preferred_element_type=F32)


def kernel(
    norm, cot_h, acts_h, pre_h, up_h, ups_h, down_h, dsc_h,
    gi_out, gu_out, gd_out,
    loc_s, loc_a, xs, xa, pre_r, act_t, wd, wu, da, dr, dpre,
    pd, td1, td2, fd, rd, farxd, nearxd, gotd, rawd, vd, faryd, nearyd, faryd2, nearyd2,
    pua, tu1a, tu2a, fua, rua, farxua, nearxua, gotua, rawua, vua, faryua, nearyua, faryu2a, nearyu2a,
    pub, tu1b, tu2b, fub, rub, farxub, nearxub, gotub, rawub, vub, faryub, nearyub, faryu2b, nearyu2b,
    gi, farz, nearz, fz, rz,
    cot, acts, pre, up, ups, down, dsc,
    sent, ssem, rsem, lsem,
):
    r, f, z = (lax.axis_index(n) for n in ("rep", "fs", "tp"))
    y = lax.div(f, 4)
    xl = lax.rem(lax.div(f, 2), 2)
    c = lax.rem(f, 2)
    x = r * 2 + xl
    oc, ox = 1 - c, 1 - xl

    def dev(dx=0, dy=0, dz=0, core=None):
        nx, ny, nz = (lax.rem(a + d + 4, 4) for a, d in ((x, dx), (y, dy), (z, dz)))
        core = c if core is None else core
        return {
            "rep": lax.div(nx, 2),
            "fs": ny * 4 + lax.rem(nx, 2) * 2 + core,
            "tp": nz,
        }

    def at(a, d):
        return lax.rem(a + d + 4, 4)

    barrier = pltpu.get_barrier_semaphore()
    peers = [dev(dz=d, core=k) for d in (1, -1) for k in (c, oc)]
    peers += [dev(dy=1), dev(dy=-1), dev(dx=1), dev(dx=-1), dev(dx=2), dev(core=oc)]
    for p in peers:
        pl.semaphore_signal(barrier, inc=1, device_id=p, device_id_type=MESH)

    loads = {}
    for i, (n, src, dst) in enumerate((
        ("down", down_h, down), ("dsc", dsc_h, dsc), ("cot", cot_h, cot), ("up", up_h, up),
        ("pre", pre_h, pre), ("acts", acts_h, acts), ("ups", ups_h, ups),
    )):
        loads[n] = pltpu.make_async_copy(src, dst, lsem.at[i])
        loads[n].start()
    started = []

    recvs = [0]

    def blank(rows):
        return sent.at[pl.ds(0, rows), :]

    def rows_in(ref):
        return math.prod(ref.shape) * jnp.dtype(ref.dtype).itemsize // 256

    class Group:
        def __init__(self):
            self.k, self.rows = recvs[0], 0
            recvs[0] += 1

        def wait_recv(self):
            d = blank(self.rows)
            pltpu.make_async_copy(d, d, rsem.at[self.k]).wait()

    def send(src, dst, to, group=None):
        group = group or Group()
        group.rows += rows_in(src)
        copy = pltpu.make_async_remote_copy(
            src_ref=src, dst_ref=dst, send_sem=ssem, recv_sem=rsem.at[group.k],
            device_id=to, device_id_type=MESH,
        )
        copy.start()
        started.append(rows_in(src))
        return group

    def split(dst, v):
        for k in range(2):
            for j in range(2):
                lanes = slice(j * 256 + k * 128, j * 256 + k * 128 + 128)
                dst[k, :, j * 128:(j + 1) * 128] = v[:, lanes]

    loads["down"].wait()
    wd[y, xl] = down[...].astype(BF)
    pl.semaphore_wait(barrier, len(peers))

    own, other = pl.ds(0, 256), pl.ds(256, 256)

    def same(ref, to, group=None):
        return send(ref, ref, to, group)

    def z_send(loc, full):
        rest = Group()

        def go(k, dz, group=None):
            part = own if k is c else other
            return send(loc.at[k], full.at[z, part, :], dev(dz=dz, core=k), group)

        first = [go(c, 1), go(oc, -1)]
        for k, dz in ((oc, 1), (c, -1), (oc, 0)):
            go(k, dz, rest)
        return first, rest

    def z_forward(full, sends):
        first, rest = sends
        first[0].wait_recv()
        same(full.at[at(z, -1), own, :], dev(dz=1), rest)
        first[1].wait_recv()
        same(full.at[at(z, 1), other, :], dev(dz=-1), rest)
        return rest

    def add(a, b):
        return a.astype(F32) + b.astype(F32)

    def relu_sq(v):
        p = jnp.maximum(v.astype(F32), 0.0)
        return (p * p).astype(BF)

    def rows_of(ref, k, xx, lo, n):
        return ref.at[k, xx, pl.ds(lo, n), :]

    yn, yp, xn, xp, zn, zp = dev(dy=1), dev(dy=-1), dev(dx=1), dev(dx=-1), dev(dz=1), dev(dz=-1)

    def x_send(w, lo, n, k, h, group=None):
        return same(rows_of(w, k, xl, lo + h * n, n), xp if h else xn, group)

    class Ring:
        def __init__(self, view, me, far, near, nxt, prv):
            self.view, self.me, self.far, self.near = view, me, far, near
            self.nxt, self.prv = nxt, prv

        def start_far(self):
            k = at(self.me, 2)
            self.f = [
                send(self.view(k, 0), self.far.at[0], self.nxt),
                send(self.view(k, 1), self.far.at[1], self.prv),
            ]

        def start_near(self):
            self.n = Group()
            send(self.view(at(self.me, 1), 1), self.near.at[0, 1], self.nxt, self.n)
            send(self.view(at(self.me, -1), 0), self.near.at[1, 0], self.prv, self.n)

        def mid(self):
            for h, d, to in ((0, 1, self.nxt), (1, -1, self.prv)):
                self.f[h].wait_recv()
                v = self.view(at(self.me, d), h)
                v[...] = add(v[...], self.far[h]).astype(BF)
                send(v, self.near.at[h, h], to, self.n)

        def result(self):
            self.n.wait_recv()
            for h in range(2):
                v = self.view(self.me, h)
                yield h, add(v[...], self.near[0, h]) + self.near[1, h].astype(F32)

    class Grad:
        def __init__(self, p, t1, t2, fin, rr, farx, nearx, got, raw, vb, fary, neary, fary2, neary2):
            n = fin.shape[0] // 2
            self.p, self.t1, self.t2, self.fin, self.rr = p, t1, t2, fin, rr
            self.got, self.raw, self.vb = got, raw, vb
            self.x1 = Ring(
                lambda k, h: p.at[pl.ds(2 * h, 2), lax.rem(k, 2), 0, lax.div(k, 2)],
                x, farx, nearx, xn, xp,
            )
            self.y1 = Ring(lambda k, h: p.at[k, h, 1], y, fary, neary, yn, yp)
            self.y2 = Ring(
                lambda k, h: t1.at[k, pl.ds(h * n, n), :], y, fary2, neary2, yn, yp
            )
            self.n = n

        def start(self):
            self.y1.start_far()
            self.x1.start_far()
            self.y1.start_near()
            self.x1.start_near()

        def mid(self):
            self.y1.mid()
            self.x1.mid()

        def second_y(self):
            for h, v in self.x1.result():
                self.t1[2 * h:2 * h + 2] = v.astype(BF)
            self.y2.start_far()
            self.y2.start_near()

        def second_x(self):
            t2, got, raw = self.t2, self.got, self.raw
            for h, v in self.y1.result():
                t2[h] = v.astype(BF)
            self.c1, self.c2 = Group(), Group()
            send(t2.at[xl, r], got.at[0], xn, self.c1)
            send(t2.at[xl, 1 - r], got.at[1], xp, self.c1)
            send(t2.at[ox, 1 - mine], raw.at[0], xn, self.c2)
            send(t2.at[ox, 1 - mine], raw.at[1], xp, self.c2)

        def second_x_mid(self):
            self.c1.wait_recv()
            v = self.t2.at[ox, mine]
            v[...] = (add(self.got[0], self.got[1]) + v[...].astype(F32)).astype(BF)
            send(v, self.vb.at[0], xn, self.c2)
            send(v, self.vb.at[1], xp, self.c2)

        def store_second(self, out):
            self.c2.wait_recv()
            out[1, 1 - r] = add(self.vb[0], self.raw[1]) * norm
            out[1, r] = add(self.vb[1], self.raw[0]) * norm

        def share(self):
            for h, v in self.y2.result():
                self.fin[h * self.n:(h + 1) * self.n, :] = v.astype(BF)
            self.g = send(self.fin, self.rr, dev(dx=2))

        def store_first(self, out):
            out[0, r] = self.fin[...].astype(F32) * norm
            self.g.wait_recv()
            out[0, 1 - r] = self.rr[...].astype(F32) * norm

    mine = r * xl + (1 - r) * ox
    gd = Grad(pd, td1, td2, fd, rd, farxd, nearxd, gotd, rawd, vd, faryd, nearyd, faryd2, nearyd2)
    ga = Grad(pua, tu1a, tu2a, fua, rua, farxua, nearxua, gotua, rawua, vua, faryua, nearyua, faryu2a, nearyu2a)
    gb = Grad(pub, tu1b, tu2b, fub, rub, farxub, nearxub, gotub, rawub, vub, faryub, nearyub, faryu2b, nearyu2b)
    scope = jax.named_scope

    with scope("a_first_sends"):
        wd1 = [
            same(rows_of(wd, y, xl, 512 * h, 512), to)
            for h, to in ((0, yn), (1, yp), (1, yn), (0, yp))
        ]
        wdx = {d: Group() for d in (0, 1, -1, 2)}
        for h in range(2):
            x_send(wd, 0, 512, y, h, wdx[0])
        loads["dsc"].wait()
        scale = dsc[:, pl.ds(pl.multiple_of(z * 512, 512), 512)]
        loads["cot"].wait()
        split(loc_s, (cot[...].astype(F32) * scale).astype(BF))
        s1 = z_send(loc_s, xs)
        xs[z, 0:256, :] = loc_s[c]
        loads["up"].wait()
        wu[y, xl] = up[...].astype(BF)
        ya, yh = Y_FIRST, Y_FIRST // 2
        xr, xh = 128 - ya, (128 - ya) // 2
        wu_x = [x_send(wu, ya, xh, y, h) for h in range(2)]
        wux = Group()
        for h in range(2):
            x_send(wu, 0, yh, y, h, wux)
        loads["pre"].wait()
        pre1 = send(pre, pre_r, dev(core=oc))
        loads["acts"].wait()
        split(loc_a, acts[...])
        xa[z, 0:256, :] = loc_a[c]
        loads["ups"].wait()
    with scope("b_wd_first"):
        wd1[0].wait_recv()
        wd2 = [same(rows_of(wd, at(y, -1), xl, 0, 512), yn)]
        x_send(wd, 0, 512, at(y, -1), 0, wdx[-1])
        wd1[1].wait_recv()
        wd2.append(same(rows_of(wd, at(y, 1), xl, 512, 512), yp))
        x_send(wd, 0, 512, at(y, 1), 1, wdx[1])
    with scope("c_z_forward"):
        s2 = z_forward(xs, s1)
        a1 = z_send(loc_a, xa)
    with scope("d_wd_second"):
        wd1[2].wait_recv()
        x_send(wd, 0, 512, at(y, -1), 1, wdx[-1])
        wd1[3].wait_recv()
        x_send(wd, 0, 512, at(y, 1), 0, wdx[1])
        wuy = [same(rows_of(wu, y, xl, 0, ya), to) for to in (yn, yp)]
        wuo = same(rows_of(wu, y, xl, ya, xr), yn)
        same(rows_of(wu, y, xl, ya, xr), yp, wux)
        wuo2 = []
        for h in range(2):
            wu_x[h].wait_recv()
            piece = rows_of(wu, y, ox, ya + xh * h, xh)
            same(piece, yn, wux)
            wuo2.append(same(piece, yp))
    with scope("e_act"):
        act_t[:, 0:256] = relu_sq(pre[...]).T
        pre1.wait_recv()
        act_t[:, 256:512] = relu_sq(pre_r[...]).T
    with scope("f_wd_third"):
        for h in range(2):
            wd2[h].wait_recv()
            x_send(wd, 0, 512, at(y, 2), h, wdx[2])
    with scope("g_scaled_wait"):
        s2.wait_recv()
    with scope("h_grad_down"):
        for k in range(4):
            part = nn(act_t[...], xs[k])
            for j in range(2):
                pd[k, j] = part[:, j * 128:(j + 1) * 128].astype(BF).reshape(2, 2, 256, 128)
        gd.y1.start_far()
        gd.x1.start_far()
        gd.x1.start_near()
    with scope("i_wu_second"):
        wuf = []
        for h, to, d in ((0, yn, -1), (1, yp, 1)):
            wuy[h].wait_recv()
            k = at(y, d)
            wuf.append(same(rows_of(wu, k, xl, yh * h, yh), to))
            x_send(wu, 0, yh, k, 0, wux)
            x_send(wu, 0, yh, k, 1, wux)
    with scope("j_acts_forward"):
        a2 = z_forward(xa, a1)
    dax = []
    for d in (0, 1, -1, 2):
        with scope("k_wd_wait"):
            wdx[d].wait_recv()
        with scope("l_d_act"):
            k = at(y, d)
            w = jnp.concatenate([wd[k, 0], wd[k, 1]], axis=1)
            for h in (0, 1):
                term = nt(xs[k, h * 256:(h + 1) * 256, :], w)
                da[h] = term if d == 0 else da[h] + term
                if d == 2:
                    dax.append(send(da.at[h], dr.at[1 - h], dev(core=oc)))
    with scope("m_wu_third"):
        wuo.wait_recv()
        same(rows_of(wu, at(y, -1), xl, ya, xr), yn, wux)
        for h in range(2):
            wuo2[h].wait_recv()
            same(rows_of(wu, at(y, 1), ox, ya + xh * h, xh), yp, wux)
        gd.y1.start_near()
    with scope("n_dpre"):
        for h in (1, 0):
            dax[1 - h].wait_recv()
            src = pre if h == 0 else pre_r
            pos = jnp.maximum(src[...].astype(F32), 0.0)
            dpre[h * 256:(h + 1) * 256, :] = (2.0 * pos * (da[h] + dr[h]) * ups[...]).astype(BF)
    with scope("o_acts_wait"):
        a2.wait_recv()
    with scope("p_grad_up"):
        for i, g in enumerate((ga, gb)):
            cols = slice(i * 512, i * 512 + 512)
            for k in range(4):
                part = nn(xa[k].T, dpre[:, cols])
                for j in range(2):
                    g.p[k, j] = part[j * 128:(j + 1) * 128, :].astype(BF).reshape(2, 2, 32, 512)
    with scope("q_gd_mid"):
        for h in range(2):
            wuf[h].wait_recv()
            x_send(wu, 0, yh, at(y, 2), h, wux)
        gd.x1.mid()
        gd.y1.mid()
        ga.start()
        gb.y1.start_far()
        gb.x1.start_far()
    zr = Ring(lambda k, h: gi.at[k, pl.ds(256 * h, 256), :], z, farz, nearz, zn, zp)
    with scope("r_wu_wait"):
        wux.wait_recv()
    with scope("s_grad_in"):
        for d in (2, 1, -1, 0):
            k = at(z, d)
            gi[k] = nt(dpre[...], wu[k].reshape(256, 1024)).astype(BF)
            if d == 2:
                zr.start_far()
            if d == -1:
                zr.start_near()
    with scope("ga_x1"):
        ga.x1.mid()
    with scope("ga_y1"):
        ga.y1.mid()
    with scope("gb_nx"):
        gb.x1.start_near()
    with scope("gb_ny"):
        gb.y1.start_near()
    with scope("gb_x1"):
        gb.x1.mid()
    with scope("u_z_mid"):
        zr.mid()
    with scope("gb_y1"):
        gb.y1.mid()
    with scope("t_y"):
        gd.second_y()
    with scope("t_x"):
        gd.second_x()
    with scope("ga_sy"):
        ga.second_y()
    with scope("ga_sx"):
        ga.second_x()
    with scope("w_gb_second_y"):
        gb.second_y()
    with scope("w_gb_second_x"):
        gb.second_x()
    with scope("v_gd_x2_mid"):
        gd.second_x_mid()
    with scope("v_gd_y2_mid"):
        gd.y2.mid()
    with scope("ga_ym"):
        ga.y2.mid()
    with scope("ga_xm"):
        ga.second_x_mid()
    with scope("y_gb_y2_mid"):
        gb.y2.mid()
    with scope("z_gd_share"):
        gd.share()
    with scope("z_ga_share"):
        ga.share()
    with scope("y_gb_x2_mid"):
        gb.second_x_mid()
    with scope("z_gb_share"):
        gb.share()
    with scope("x_gi"):
        for h, v in zr.result():
            fz[h] = v.astype(BF)
        gx = send(fz.at[1], rz, dev(core=oc))
    with scope("zc_gi_out"):
        gx.wait_recv()
        for j in range(2):
            lanes = pl.ds(pl.multiple_of(j * 256 + c * 128, 128), 128)
            gi_out[:, lanes] = fz[0, :, j * 128:(j + 1) * 128]
            lanes = pl.ds(pl.multiple_of(j * 256 + oc * 128, 128), 128)
            gi_out[:, lanes] = rz[:, j * 128:(j + 1) * 128]
    outs = [(gd, gd_out)] + [(g, gu_out.at[:, :, :, pl.ds(i * 512, 512)]) for i, g in ((0, ga), (1, gb))]
    with scope("ze_second_out"):
        for g, out in outs:
            g.store_second(out)
    with scope("zf_first_out"):
        for g, out in outs:
            g.store_first(out)
    with scope("zh_drain"):
        assert recvs[0] == RECVS and sum(started) == SENT_ROWS, (recvs, sum(started))
        pltpu.make_async_copy(sent, sent, ssem).wait()


def write_out(a, b, c, x, y, z, sems):
    copies = [
        pltpu.make_async_copy(v, w, sems.at[i])
        for i, (v, w) in enumerate(((a, x), (b, y), (c, z)))
    ]
    for k in copies:
        k.start()
    for k in copies:
        k.wait()


def body(acts, cotangent, pre_act, up_store, up_scale, down_store, down_scale):
    tokens = acts.shape[0] * lax.axis_size("fs") * lax.axis_size("rep")
    norm = 1.0 / math.sqrt(tokens)

    def vm(*shape, dtype=BF):
        return pltpu.VMEM(shape, dtype)

    def grad_bufs(n, m):
        return [
            vm(4, 2, 2, 2, n, m), vm(4, n, m), vm(2, 2, n, m), vm(n, m), vm(n, m),
            vm(2, 2, n, m), vm(2, 2, 2, n, m), vm(2, n, m), vm(2, n, m), vm(2, n, m),
            vm(2, 2, n, m), vm(2, 2, 2, n, m), vm(2, n // 2, m), vm(2, 2, n // 2, m),
        ]

    spec = pl.BlockSpec(memory_space=pltpu.VMEM)

    def call(*args):
        return kernel(norm, *args)

    gi, gu, gd = pl.pallas_call(
        call,
        name="ffn_backward",
        out_shape=(
            pltpu.VMEM((256, 512), BF),
            pltpu.VMEM((2, 2, 32, 1024), F32),
            pltpu.VMEM((2, 2, 256, 128), F32),
        ),
        in_specs=[pl.BlockSpec(memory_space=pl.ANY)] * 7,
        out_specs=(spec,) * 3,
        scratch_shapes=[
            vm(2, 256, 256), vm(2, 256, 256), vm(4, 512, 256), vm(4, 512, 256),
            vm(256, 1024), vm(1024, 512), vm(4, 2, 1024, 128), vm(4, 2, 128, 1024),
            vm(2, 256, 1024, dtype=F32), vm(2, 256, 1024, dtype=F32), vm(512, 1024),
            *grad_bufs(256, 128),
            *grad_bufs(32, 512),
            *grad_bufs(32, 512),
            vm(4, 512, 256), vm(2, 256, 256), vm(2, 2, 256, 256), vm(2, 256, 256), vm(256, 256),
            vm(256, 512), vm(256, 512), vm(256, 1024), vm(128, 1024, dtype=F32),
            vm(1, 1024, dtype=F32), vm(1024, 128, dtype=F32), vm(1, 2048, dtype=F32),
            vm(SENT_ROWS, 128),
            pltpu.SemaphoreType.DMA,
            pltpu.SemaphoreType.DMA((RECVS,)),
            pltpu.SemaphoreType.DMA((7,)),
        ],
        compiler_params=pltpu.CompilerParams(
            collective_id=0, has_side_effects=True, vmem_limit_bytes=56 * 1024 * 1024
        ),
    )(
        cotangent, acts, pre_act, up_store, up_scale.reshape(1, -1),
        down_store, down_scale.reshape(1, -1),
    )
    outs = [pltpu.with_memory_space_constraint(v, pltpu.VMEM) for v in (gi, gu, gd)]
    gi, gu, gd = pl.pallas_call(
        write_out,
        name="write_out",
        out_shape=tuple(jax.ShapeDtypeStruct(v.shape, v.dtype) for v in outs),
        in_specs=[spec] * 3,
        out_specs=(pl.BlockSpec(memory_space=pl.ANY),) * 3,
        scratch_shapes=[pltpu.SemaphoreType.DMA((3,))],
    )(*outs)
    return gi, gu.reshape(up_store.shape), gd.reshape(down_store.shape)


def solution(mesh):
    return jax.shard_map(
        body,
        mesh=mesh,
        in_specs=(
            P(("rep", "fs"), "tp"),
            P(("rep", "fs"), "tp"),
            P(("rep", "fs"), "tp"),
            P("fs", "tp"),
            P("tp"),
            P("tp", "fs"),
            P(),
        ),
        out_specs=(P(("rep", "fs"), "tp"), P("fs", "tp"), P("tp", "fs")),
        check_vma=False,
    )
```

```python
import math

import jax
import jax.numpy as jnp
from jax import lax
from jax.experimental import pallas as pl
from jax.experimental.pallas import tpu as pltpu
from jax.sharding import PartitionSpec as P

BF = jnp.bfloat16
F32 = jnp.float32
MESH = pl.DeviceIdType.MESH
RECVS = 69
Y_FIRST = 64
SENT_ROWS = 52736


def nt(a, b):
    return lax.dot_general(a, b, (((1,), (1,)), ((), ())), preferred_element_type=F32)


def nn(a, b):
    return lax.dot_general(a, b, (((1,), (0,)), ((), ())), preferred_element_type=F32)


def kernel(
    norm, cot_h, acts_h, pre_h, up_h, ups_h, down_h, dsc_h,
    gi_out, gu_out, gd_out,
    loc_s, loc_a, xs, xa, pre_r, act_t, wd, wu, da, dr, dpre,
    pd, td1, td2, fd, rd, farxd, nearxd, gotd, rawd, vd, faryd, nearyd, faryd2, nearyd2,
    pua, tu1a, tu2a, fua, rua, farxua, nearxua, gotua, rawua, vua, faryua, nearyua, faryu2a, nearyu2a,
    pub, tu1b, tu2b, fub, rub, farxub, nearxub, gotub, rawub, vub, faryub, nearyub, faryu2b, nearyu2b,
    gi, farz, nearz, fz, rz,
    cot, acts, pre, up, ups, down, dsc,
    sent, ssem, rsem, lsem,
):
    r, f, z = (lax.axis_index(n) for n in ("rep", "fs", "tp"))
    y = lax.div(f, 4)
    xl = lax.rem(lax.div(f, 2), 2)
    c = lax.rem(f, 2)
    x = r * 2 + xl
    oc, ox = 1 - c, 1 - xl

    def dev(dx=0, dy=0, dz=0, core=None):
        nx, ny, nz = (lax.rem(a + d + 4, 4) for a, d in ((x, dx), (y, dy), (z, dz)))
        core = c if core is None else core
        return {
            "rep": lax.div(nx, 2),
            "fs": ny * 4 + lax.rem(nx, 2) * 2 + core,
            "tp": nz,
        }

    def at(a, d):
        return lax.rem(a + d + 4, 4)

    barrier = pltpu.get_barrier_semaphore()
    peers = [dev(dz=d, core=k) for d in (1, -1) for k in (c, oc)]
    peers += [dev(dy=1), dev(dy=-1), dev(dx=1), dev(dx=-1), dev(dx=2), dev(core=oc)]
    for p in peers:
        pl.semaphore_signal(barrier, inc=1, device_id=p, device_id_type=MESH)

    loads = {}
    for i, (n, src, dst) in enumerate((
        ("down", down_h, down), ("dsc", dsc_h, dsc), ("cot", cot_h, cot), ("up", up_h, up),
        ("pre", pre_h, pre), ("acts", acts_h, acts), ("ups", ups_h, ups),
    )):
        loads[n] = pltpu.make_async_copy(src, dst, lsem.at[i])
        loads[n].start()
    started = []

    recvs = [0]

    def blank(rows):
        return sent.at[pl.ds(0, rows), :]

    def rows_in(ref):
        return math.prod(ref.shape) * jnp.dtype(ref.dtype).itemsize // 256

    class Group:
        def __init__(self):
            self.k, self.rows = recvs[0], 0
            recvs[0] += 1

        def wait_recv(self):
            d = blank(self.rows)
            pltpu.make_async_copy(d, d, rsem.at[self.k]).wait()

    def send(src, dst, to, group=None):
        group = group or Group()
        group.rows += rows_in(src)
        copy = pltpu.make_async_remote_copy(
            src_ref=src, dst_ref=dst, send_sem=ssem, recv_sem=rsem.at[group.k],
            device_id=to, device_id_type=MESH,
        )
        copy.start()
        started.append(rows_in(src))
        return group

    def split(dst, v):
        for k in range(2):
            for j in range(2):
                lanes = slice(j * 256 + k * 128, j * 256 + k * 128 + 128)
                dst[k, :, j * 128:(j + 1) * 128] = v[:, lanes]

    loads["down"].wait()
    wd[y, xl] = down[...].astype(BF)
    pl.semaphore_wait(barrier, len(peers))

    own, other = pl.ds(0, 256), pl.ds(256, 256)

    def same(ref, to, group=None):
        return send(ref, ref, to, group)

    def z_send(loc, full):
        rest = Group()

        def go(k, dz, group=None):
            part = own if k is c else other
            return send(loc.at[k], full.at[z, part, :], dev(dz=dz, core=k), group)

        first = [go(c, 1), go(oc, -1)]
        for k, dz in ((oc, 1), (c, -1), (oc, 0)):
            go(k, dz, rest)
        return first, rest

    def z_forward(full, sends):
        first, rest = sends
        first[0].wait_recv()
        same(full.at[at(z, -1), own, :], dev(dz=1), rest)
        first[1].wait_recv()
        same(full.at[at(z, 1), other, :], dev(dz=-1), rest)
        return rest

    def add(a, b):
        return a.astype(F32) + b.astype(F32)

    def relu_sq(v):
        p = jnp.maximum(v.astype(F32), 0.0)
        return (p * p).astype(BF)

    def rows_of(ref, k, xx, lo, n):
        return ref.at[k, xx, pl.ds(lo, n), :]

    yn, yp, xn, xp, zn, zp = dev(dy=1), dev(dy=-1), dev(dx=1), dev(dx=-1), dev(dz=1), dev(dz=-1)

    def x_send(w, lo, n, k, h, group=None):
        return same(rows_of(w, k, xl, lo + h * n, n), xp if h else xn, group)

    class Ring:
        def __init__(self, view, me, far, near, nxt, prv):
            self.view, self.me, self.far, self.near = view, me, far, near
            self.nxt, self.prv = nxt, prv

        def start_far(self):
            k = at(self.me, 2)
            self.f = [
                send(self.view(k, 0), self.far.at[0], self.nxt),
                send(self.view(k, 1), self.far.at[1], self.prv),
            ]

        def start_near(self):
            self.n = Group()
            send(self.view(at(self.me, 1), 1), self.near.at[0, 1], self.nxt, self.n)
            send(self.view(at(self.me, -1), 0), self.near.at[1, 0], self.prv, self.n)

        def mid(self):
            for h, d, to in ((0, 1, self.nxt), (1, -1, self.prv)):
                self.f[h].wait_recv()
                v = self.view(at(self.me, d), h)
                v[...] = add(v[...], self.far[h]).astype(BF)
                send(v, self.near.at[h, h], to, self.n)

        def result(self):
            self.n.wait_recv()
            for h in range(2):
                v = self.view(self.me, h)
                yield h, add(v[...], self.near[0, h]) + self.near[1, h].astype(F32)

    class Grad:
        def __init__(self, p, t1, t2, fin, rr, farx, nearx, got, raw, vb, fary, neary, fary2, neary2):
            n = fin.shape[0] // 2
            self.p, self.t1, self.t2, self.fin, self.rr = p, t1, t2, fin, rr
            self.got, self.raw, self.vb = got, raw, vb
            self.x1 = Ring(
                lambda k, h: p.at[pl.ds(2 * h, 2), lax.rem(k, 2), 0, lax.div(k, 2)],
                x, farx, nearx, xn, xp,
            )
            self.y1 = Ring(lambda k, h: p.at[k, h, 1], y, fary, neary, yn, yp)
            self.y2 = Ring(
                lambda k, h: t1.at[k, pl.ds(h * n, n), :], y, fary2, neary2, yn, yp
            )
            self.n = n

        def start(self):
            self.y1.start_far()
            self.x1.start_far()
            self.y1.start_near()
            self.x1.start_near()

        def mid(self):
            self.y1.mid()
            self.x1.mid()

        def second_y(self):
            for h, v in self.x1.result():
                self.t1[2 * h:2 * h + 2] = v.astype(BF)
            self.y2.start_far()
            self.y2.start_near()

        def second_x(self):
            t2, got, raw = self.t2, self.got, self.raw
            for h, v in self.y1.result():
                t2[h] = v.astype(BF)
            self.c1, self.c2 = Group(), Group()
            send(t2.at[xl, r], got.at[0], xn, self.c1)
            send(t2.at[xl, 1 - r], got.at[1], xp, self.c1)
            send(t2.at[ox, 1 - mine], raw.at[0], xn, self.c2)
            send(t2.at[ox, 1 - mine], raw.at[1], xp, self.c2)

        def second_x_mid(self):
            self.c1.wait_recv()
            v = self.t2.at[ox, mine]
            v[...] = (add(self.got[0], self.got[1]) + v[...].astype(F32)).astype(BF)
            send(v, self.vb.at[0], xn, self.c2)
            send(v, self.vb.at[1], xp, self.c2)

        def store_second(self, out):
            self.c2.wait_recv()
            out[1, 1 - r] = add(self.vb[0], self.raw[1]) * norm
            out[1, r] = add(self.vb[1], self.raw[0]) * norm

        def share(self):
            for h, v in self.y2.result():
                self.fin[h * self.n:(h + 1) * self.n, :] = v.astype(BF)
            self.g = send(self.fin, self.rr, dev(dx=2))

        def store_first(self, out):
            out[0, r] = self.fin[...].astype(F32) * norm
            self.g.wait_recv()
            out[0, 1 - r] = self.rr[...].astype(F32) * norm

    mine = r * xl + (1 - r) * ox
    gd = Grad(pd, td1, td2, fd, rd, farxd, nearxd, gotd, rawd, vd, faryd, nearyd, faryd2, nearyd2)
    ga = Grad(pua, tu1a, tu2a, fua, rua, farxua, nearxua, gotua, rawua, vua, faryua, nearyua, faryu2a, nearyu2a)
    gb = Grad(pub, tu1b, tu2b, fub, rub, farxub, nearxub, gotub, rawub, vub, faryub, nearyub, faryu2b, nearyu2b)
    scope = jax.named_scope

    with scope("a_first_sends"):
        wd1 = [
            same(rows_of(wd, y, xl, 512 * h, 512), to)
            for h, to in ((0, yn), (1, yp), (1, yn), (0, yp))
        ]
        wdx = {d: Group() for d in (0, 1, -1, 2)}
        for h in range(2):
            x_send(wd, 0, 512, y, h, wdx[0])
        loads["dsc"].wait()
        scale = dsc[:, pl.ds(pl.multiple_of(z * 512, 512), 512)]
        loads["cot"].wait()
        split(loc_s, (cot[...].astype(F32) * scale).astype(BF))
        s1 = z_send(loc_s, xs)
        xs[z, 0:256, :] = loc_s[c]
        loads["up"].wait()
        wu[y, xl] = up[...].astype(BF)
        ya, yh = Y_FIRST, Y_FIRST // 2
        xr, xh = 128 - ya, (128 - ya) // 2
        wu_x = [x_send(wu, ya, xh, y, h) for h in range(2)]
        wux = Group()
        for h in range(2):
            x_send(wu, 0, yh, y, h, wux)
        loads["pre"].wait()
        pre1 = send(pre, pre_r, dev(core=oc))
        loads["acts"].wait()
        split(loc_a, acts[...])
        xa[z, 0:256, :] = loc_a[c]
        loads["ups"].wait()
    with scope("b_wd_first"):
        wd1[0].wait_recv()
        wd2 = [same(rows_of(wd, at(y, -1), xl, 0, 512), yn)]
        x_send(wd, 0, 512, at(y, -1), 0, wdx[-1])
        wd1[1].wait_recv()
        wd2.append(same(rows_of(wd, at(y, 1), xl, 512, 512), yp))
        x_send(wd, 0, 512, at(y, 1), 1, wdx[1])
    with scope("c_z_forward"):
        s2 = z_forward(xs, s1)
        a1 = z_send(loc_a, xa)
    with scope("d_wd_second"):
        wd1[2].wait_recv()
        x_send(wd, 0, 512, at(y, -1), 1, wdx[-1])
        wd1[3].wait_recv()
        x_send(wd, 0, 512, at(y, 1), 0, wdx[1])
        wuy = [same(rows_of(wu, y, xl, 0, ya), to) for to in (yn, yp)]
        wuo = same(rows_of(wu, y, xl, ya, xr), yn)
        same(rows_of(wu, y, xl, ya, xr), yp, wux)
        wuo2 = []
        for h in range(2):
            wu_x[h].wait_recv()
            piece = rows_of(wu, y, ox, ya + xh * h, xh)
            same(piece, yn, wux)
            wuo2.append(same(piece, yp))
    with scope("e_act"):
        act_t[:, 0:256] = relu_sq(pre[...]).T
        pre1.wait_recv()
        act_t[:, 256:512] = relu_sq(pre_r[...]).T
    with scope("f_wd_third"):
        for h in range(2):
            wd2[h].wait_recv()
            x_send(wd, 0, 512, at(y, 2), h, wdx[2])
    with scope("g_scaled_wait"):
        s2.wait_recv()
    with scope("h_grad_down"):
        for k in range(4):
            part = nn(act_t[...], xs[k])
            for j in range(2):
                pd[k, j] = part[:, j * 128:(j + 1) * 128].astype(BF).reshape(2, 2, 256, 128)
        gd.x1.start_far()
        gd.x1.start_near()
    with scope("i_wu_second"):
        wuf = []
        for h, to, d in ((0, yn, -1), (1, yp, 1)):
            wuy[h].wait_recv()
            k = at(y, d)
            wuf.append(same(rows_of(wu, k, xl, yh * h, yh), to))
            x_send(wu, 0, yh, k, 0, wux)
            x_send(wu, 0, yh, k, 1, wux)
        gd.y1.start_far()
    with scope("j_acts_forward"):
        a2 = z_forward(xa, a1)
    dax = []
    for d in (0, 1, -1, 2):
        with scope("k_wd_wait"):
            wdx[d].wait_recv()
        with scope("l_d_act"):
            k = at(y, d)
            w = jnp.concatenate([wd[k, 0], wd[k, 1]], axis=1)
            for h in (0, 1):
                term = nt(xs[k, h * 256:(h + 1) * 256, :], w)
                da[h] = term if d == 0 else da[h] + term
                if d == 2:
                    dax.append(send(da.at[h], dr.at[1 - h], dev(core=oc)))
    with scope("m_wu_third"):
        wuo.wait_recv()
        same(rows_of(wu, at(y, -1), xl, ya, xr), yn, wux)
        for h in range(2):
            wuo2[h].wait_recv()
            same(rows_of(wu, at(y, 1), ox, ya + xh * h, xh), yp, wux)
        gd.y1.start_near()
    with scope("m_x_sends"):
        for h in range(2):
            wuf[h].wait_recv()
            x_send(wu, 0, yh, at(y, 2), h, wux)
        gd.x1.mid()
    with scope("n_dpre"):
        for h in (1, 0):
            dax[1 - h].wait_recv()
            src = pre if h == 0 else pre_r
            pos = jnp.maximum(src[...].astype(F32), 0.0)
            dpre[h * 256:(h + 1) * 256, :] = (2.0 * pos * (da[h] + dr[h]) * ups[...]).astype(BF)
    with scope("o_acts_wait"):
        a2.wait_recv()
    with scope("p_grad_up"):
        for i, g in enumerate((ga, gb)):
            cols = slice(i * 512, i * 512 + 512)
            for k in range(4):
                part = nn(xa[k].T, dpre[:, cols])
                for j in range(2):
                    g.p[k, j] = part[j * 128:(j + 1) * 128, :].astype(BF).reshape(2, 2, 32, 512)
    with scope("q_gd_mid"):
        gd.y1.mid()
        ga.start()
        gb.y1.start_far()
        gb.x1.start_far()
    zr = Ring(lambda k, h: gi.at[k, pl.ds(256 * h, 256), :], z, farz, nearz, zn, zp)
    with scope("r_wu_wait"):
        wux.wait_recv()
    with scope("s_grad_in"):
        for d in (2, 1, -1, 0):
            k = at(z, d)
            gi[k] = nt(dpre[...], wu[k].reshape(256, 1024)).astype(BF)
            if d == 2:
                zr.start_far()
            if d == -1:
                zr.start_near()
    with scope("ga_x1"):
        ga.x1.mid()
    with scope("ga_y1"):
        ga.y1.mid()
    with scope("gb_nx"):
        gb.x1.start_near()
    with scope("gb_ny"):
        gb.y1.start_near()
    with scope("gb_x1"):
        gb.x1.mid()
    with scope("u_z_mid"):
        zr.mid()
    with scope("gb_y1"):
        gb.y1.mid()
    with scope("t_y"):
        gd.second_y()
    with scope("t_x"):
        gd.second_x()
    with scope("ga_sy"):
        ga.second_y()
    with scope("ga_sx"):
        ga.second_x()
    with scope("w_gb_second_y"):
        gb.second_y()
    with scope("w_gb_second_x"):
        gb.second_x()
    with scope("v_gd_x2_mid"):
        gd.second_x_mid()
    with scope("v_gd_y2_mid"):
        gd.y2.mid()
    with scope("ga_ym"):
        ga.y2.mid()
    with scope("ga_xm"):
        ga.second_x_mid()
    with scope("y_gb_y2_mid"):
        gb.y2.mid()
    with scope("z_gd_share"):
        gd.share()
    with scope("z_ga_share"):
        ga.share()
    with scope("y_gb_x2_mid"):
        gb.second_x_mid()
    with scope("z_gb_share"):
        gb.share()
    with scope("x_gi"):
        for h, v in zr.result():
            fz[h] = v.astype(BF)
        gx = send(fz.at[1], rz, dev(core=oc))
    with scope("zc_gi_out"):
        gx.wait_recv()
        for j in range(2):
            lanes = pl.ds(pl.multiple_of(j * 256 + c * 128, 128), 128)
            gi_out[:, lanes] = fz[0, :, j * 128:(j + 1) * 128]
            lanes = pl.ds(pl.multiple_of(j * 256 + oc * 128, 128), 128)
            gi_out[:, lanes] = rz[:, j * 128:(j + 1) * 128]
    outs = [(gd, gd_out)] + [(g, gu_out.at[:, :, :, pl.ds(i * 512, 512)]) for i, g in ((0, ga), (1, gb))]
    with scope("ze_second_out"):
        for g, out in outs:
            g.store_second(out)
    with scope("zf_first_out"):
        for g, out in outs:
            g.store_first(out)
    with scope("zh_drain"):
        assert recvs[0] == RECVS and sum(started) == SENT_ROWS, (recvs, sum(started))
        pltpu.make_async_copy(sent, sent, ssem).wait()


def write_out(a, b, c, x, y, z, sems):
    copies = [
        pltpu.make_async_copy(v, w, sems.at[i])
        for i, (v, w) in enumerate(((a, x), (b, y), (c, z)))
    ]
    for k in copies:
        k.start()
    for k in copies:
        k.wait()


def body(acts, cotangent, pre_act, up_store, up_scale, down_store, down_scale):
    tokens = acts.shape[0] * lax.axis_size("fs") * lax.axis_size("rep")
    norm = 1.0 / math.sqrt(tokens)

    def vm(*shape, dtype=BF):
        return pltpu.VMEM(shape, dtype)

    def grad_bufs(n, m):
        return [
            vm(4, 2, 2, 2, n, m), vm(4, n, m), vm(2, 2, n, m), vm(n, m), vm(n, m),
            vm(2, 2, n, m), vm(2, 2, 2, n, m), vm(2, n, m), vm(2, n, m), vm(2, n, m),
            vm(2, 2, n, m), vm(2, 2, 2, n, m), vm(2, n // 2, m), vm(2, 2, n // 2, m),
        ]

    spec = pl.BlockSpec(memory_space=pltpu.VMEM)

    def call(*args):
        return kernel(norm, *args)

    gi, gu, gd = pl.pallas_call(
        call,
        name="ffn_backward",
        out_shape=(
            pltpu.VMEM((256, 512), BF),
            pltpu.VMEM((2, 2, 32, 1024), F32),
            pltpu.VMEM((2, 2, 256, 128), F32),
        ),
        in_specs=[pl.BlockSpec(memory_space=pl.ANY)] * 7,
        out_specs=(spec,) * 3,
        scratch_shapes=[
            vm(2, 256, 256), vm(2, 256, 256), vm(4, 512, 256), vm(4, 512, 256),
            vm(256, 1024), vm(1024, 512), vm(4, 2, 1024, 128), vm(4, 2, 128, 1024),
            vm(2, 256, 1024, dtype=F32), vm(2, 256, 1024, dtype=F32), vm(512, 1024),
            *grad_bufs(256, 128),
            *grad_bufs(32, 512),
            *grad_bufs(32, 512),
            vm(4, 512, 256), vm(2, 256, 256), vm(2, 2, 256, 256), vm(2, 256, 256), vm(256, 256),
            vm(256, 512), vm(256, 512), vm(256, 1024), vm(128, 1024, dtype=F32),
            vm(1, 1024, dtype=F32), vm(1024, 128, dtype=F32), vm(1, 2048, dtype=F32),
            vm(SENT_ROWS, 128),
            pltpu.SemaphoreType.DMA,
            pltpu.SemaphoreType.DMA((RECVS,)),
            pltpu.SemaphoreType.DMA((7,)),
        ],
        compiler_params=pltpu.CompilerParams(
            collective_id=0, has_side_effects=True, vmem_limit_bytes=56 * 1024 * 1024
        ),
    )(
        cotangent, acts, pre_act, up_store, up_scale.reshape(1, -1),
        down_store, down_scale.reshape(1, -1),
    )
    outs = [pltpu.with_memory_space_constraint(v, pltpu.VMEM) for v in (gi, gu, gd)]
    gi, gu, gd = pl.pallas_call(
        write_out,
        name="write_out",
        out_shape=tuple(jax.ShapeDtypeStruct(v.shape, v.dtype) for v in outs),
        in_specs=[spec] * 3,
        out_specs=(pl.BlockSpec(memory_space=pl.ANY),) * 3,
        scratch_shapes=[pltpu.SemaphoreType.DMA((3,))],
    )(*outs)
    return gi, gu.reshape(up_store.shape), gd.reshape(down_store.shape)


def solution(mesh):
    return jax.shard_map(
        body,
        mesh=mesh,
        in_specs=(
            P(("rep", "fs"), "tp"),
            P(("rep", "fs"), "tp"),
            P(("rep", "fs"), "tp"),
            P("fs", "tp"),
            P("tp"),
            P("tp", "fs"),
            P(),
        ),
        out_specs=(P(("rep", "fs"), "tp"), P("fs", "tp"), P("tp", "fs")),
        check_vma=False,
    )
```
